32 devices in a mesh: sp: 8 (over z, x), tp: 4 (over y, core).
Axes of the slice: x: 2, y: 2, z: 4, core: 2. Of those that a mesh axis runs over, the one named last changes fastest.
Arguments:
- glu_value: bfloat16 [1024, 2048], P('tp', 'sp')
- glu_gate: bfloat16 [1024, 2048], P('tp', 'sp'), may hold values from -8 to 8
- conv_taps: float32 [1024, 31], P('tp'), may hold values from -1 to 1
- norm_gain: float32 [1024], P('tp'), may hold values from 0.1 to 1.9
- out_proj: bfloat16 [1024, 2048], P(None, 'tp'), may hold values from -0.1875 to 0.1875
- resid: bfloat16 [2048, 2048], P('sp', 'tp'), may hold values from -6 to 6
- expert_ids: int32 [2048, 2], P('sp'), may hold values from 0 to 7, all different within a row; in each aligned block of 256 rows (0 to 255, 256 to 511, ...) at most 128 rows name the same one
- route_logits: float32 [2048, 2], P('sp'), may hold values from -8 to 8
- group_prob: float32 [2048], P('sp'), may hold values from 0.2 to 1
- w_gate: bfloat16 [8, 2048, 4096], P('sp', None, 'tp'), may hold values from -0.125 to 0.125
- w_up: bfloat16 [8, 2048, 4096], P('sp', None, 'tp'), may hold values from -0.125 to 0.125
- w_down: bfloat16 [8, 4096, 2048], P('sp', None, 'tp'), may hold values from -0.09375 to 0.09375
Outputs:
- layer_out: bfloat16 [2048, 2048], P('sp', 'tp')
The draws below stay inside these ranges and needn't reach their ends.
Inputs may be any that keep to these rules, and one draw needn't show every extreme that they name: `expert_ids`: each row names 2 different experts. In each aligned block of 256 rows (the rows of one index of sp) no expert is named by more than 128 rows, a bound that some block reaches.
All inputs are finite; a program needn't handle non-finite values.
Results may differ from the reference program's by a relative error of at most 0.0061.
Values may be sent and summed in bfloat16 or wider, within the bound.
A program may use at most 64 MiB of HBM per device.

```python
import math
import jax
import jax.numpy as jnp
import numpy as np
from jax import lax

D = 2048
CH = 1024
FF = 4096
KW = 31
TOPK = 2
TOK_DEV = 256
TOKENS = 2048
EXPERTS = 8
CAP = 128
N_SP = 8


def draw_glu_value(key, part):
    keyset = jax.random.split(key, 2)
    position = jnp.arange(CH, dtype=jnp.float32) / CH
    column = 10.0 ** position * jax.random.uniform(keyset[1], (CH,), jnp.float32, 0.5, 1.5)
    sample = jax.random.normal(keyset[0], (CH, TOKENS), jnp.float32)
    return (sample * column[:, None]).astype(jnp.bfloat16)


def block_scale(own_key, extent, cuts, smallest, largest):
    loudness = 1.0
    for axis_at, parts in cuts:
        steps = jax.random.uniform(jax.random.fold_in(jax.random.fold_in(own_key, 6), axis_at), (parts,), jnp.float32, smallest / len(cuts), largest / len(cuts))
        loudness = loudness * jnp.repeat(jnp.exp(steps), extent[axis_at] // parts).reshape((-1,) + (1,) * (len(extent) - 1 - axis_at))
    return loudness


def routed_block(rng, own, number, rows, amount, top, bound, slope):
    order = jax.random.permutation(rng, amount)
    packed, usual = shares(amount, rows * top, bound, slope, True), shares(amount, rows * top, bound, slope, False)
    places = jnp.arange(amount)

    def named(sizes, rotation):
        used = int((sizes > 0).sum())
        fixed = max(1, used // 4)
        passed = fixed + (places - fixed + rotation * (used - fixed)) % max(1, amount - fixed)
        return jnp.zeros((amount,), jnp.int32).at[order[jnp.where(places < fixed, places, passed)]].set(jnp.asarray(sizes, jnp.int32))

    sizes = jnp.where(number % 4 == 0, named(packed, number // 4), named(usual, number - number // 4 - 1))
    mixed = jax.random.permutation(jax.random.fold_in(own, 3), amount)
    donor, sink = mixed[0:amount // 2 * 2:2], mixed[1:amount // 2 * 2:2]
    margin = jnp.minimum(sizes[donor] - 1, bound - sizes[sink]) // 2
    margin = jnp.where((donor == order[0]) | (sink == order[0]) | (sizes[sink] == 0), 0, jnp.maximum(margin, 0))
    passed = jax.random.randint(jax.random.fold_in(own, 4), (amount // 2,), 0, 1 << 20) % (margin + 1)
    sizes = sizes.at[donor].add(-passed).at[sink].add(passed)
    members = jnp.searchsorted(jnp.cumsum(sizes), jnp.arange(rows * top), side="right").astype(jnp.int32)
    listing = members.reshape(top, rows).T
    listing = listing[jax.random.permutation(jax.random.fold_in(own, 1), rows)]
    rotation = jax.random.randint(jax.random.fold_in(own, 2), (rows, 1), 0, top)
    return jnp.take_along_axis(listing, (jnp.arange(top)[None, :] + rotation) % top, axis=1)


def shares(count, total, reach, slope, full):
    portions = [(1 << 20) // math.isqrt(rank ** slope) + 1 for rank in range(1, count + 1)]
    largest = reach if full else min(reach, max(-(-total // count), total * portions[0] // sum(portions)))
    least = 1 if total - largest >= count - 1 else 0
    holding, surplus = [largest] + [least] * (count - 1), total - largest - least * (count - 1)
    while surplus > 0:
        free = [i for i in range(1, count) if holding[i] < largest] or [i for i in range(1, count) if holding[i] < reach]
        pool, left = sum([portions[i] for i in free]), surplus
        for i in free:
            more = min(reach - holding[i], max(1, left * portions[i] // pool), surplus)
            holding[i] = holding[i] + more
            surplus = surplus - more
    return np.array(holding)


def scatter_about(rng, dims, scale, most, shards=(), kind=jnp.bfloat16):
    entries = scale * jax.random.normal(rng, dims, jnp.float32)
    if shards:
        entries = entries * block_scale(rng, dims, shards, -0.22, 0.18)
    return jnp.clip(entries, -most, most).astype(kind)


def setup_inputs(seed: int = 0) -> dict:
    key_list = jax.random.split(jax.random.key(seed), 13)
    glu_value = draw_glu_value(jax.random.fold_in(key_list[12], 71), 0)
    glu_gate = scatter_about(key_list[1], (CH, TOKENS), 1.5, 8.0, ((0, 4), (1, 8)))
    conv_taps = scatter_about(key_list[2], (CH, KW), KW ** -0.5, 1.0, ((0, 4),), jnp.float32)
    norm_gain = jnp.clip(1.0 + 0.18 * jax.random.normal(key_list[3], (CH,), jnp.float32), 0.1, 1.9)
    out_proj = scatter_about(key_list[4], (CH, D), CH ** -0.5, 0.1875, ((1, 4),))
    resid = scatter_about(key_list[5], (TOKENS, D), 1.0, 6.0, ((0, 8), (1, 4)))
    expert_ids_keys = jax.random.split(jax.random.fold_in(key_list[6], 1), TOKENS // TOK_DEV)
    expert_ids_turns = jax.random.permutation(jax.random.fold_in(key_list[6], 3), TOKENS // TOK_DEV)
    expert_ids = jax.vmap(lambda own, number: routed_block(jax.random.fold_in(key_list[6], 2), own, number, TOK_DEV, EXPERTS, TOPK, CAP, 2))(expert_ids_keys, expert_ids_turns).reshape((TOKENS, TOPK))
    route_logits = scatter_about(key_list[7], (TOKENS, TOPK), 1.5, 8.0, ((0, 8),), jnp.float32)
    group_prob = jnp.clip(jnp.exp(math.log(1.0) - 1.609438 * jax.random.uniform(key_list[8], (TOKENS,), jnp.float32) ** block_scale(key_list[8], (TOKENS,), ((0, 8),), -0.2, 0.2)), 0.2, 1.0)
    w_gate = scatter_about(key_list[9], (EXPERTS, D, FF), D ** -0.5, 0.125, ((0, 8), (2, 4)))
    w_up = scatter_about(key_list[10], (EXPERTS, D, FF), D ** -0.5, 0.125, ((0, 8), (2, 4)))
    w_down = scatter_about(key_list[11], (EXPERTS, FF, D), FF ** -0.5, 0.09375, ((0, 8), (2, 4)))
    return dict(glu_value=glu_value, glu_gate=glu_gate, conv_taps=conv_taps, norm_gain=norm_gain, out_proj=out_proj, resid=resid, expert_ids=expert_ids, route_logits=route_logits, group_prob=group_prob, w_gate=w_gate, w_up=w_up, w_down=w_down)


def reference(glu_value, glu_gate, conv_taps, norm_gain, out_proj, resid, expert_ids, route_logits, group_prob, w_gate, w_up, w_down):
    gated = (glu_value.astype(jnp.float32) * jax.nn.sigmoid(glu_gate.astype(jnp.float32))).astype(jnp.bfloat16)
    padded = jnp.pad(gated.astype(jnp.float32), ((0, 0), (KW - 1, 0)))
    filtered = jnp.zeros((CH, TOKENS), jnp.float32)
    for offset in range(KW):
        filtered = filtered + conv_taps[:, offset:offset + 1] * padded[:, offset:offset + TOKENS]
    mean = lax.optimization_barrier(jnp.sum(filtered, axis=0)) / CH
    meansq = lax.optimization_barrier(jnp.sum(filtered * filtered, axis=0)) / CH
    var = meansq - mean * mean
    normed = (filtered - mean[None, :]) * lax.rsqrt(var[None, :] + 1e-05) * norm_gain[:, None]
    activated = jax.nn.silu(normed).astype(jnp.bfloat16)
    projected = lax.dot_general(activated, out_proj, (((0,), (0,)), ((), ())), preferred_element_type=jnp.float32)
    mixed = (resid.astype(jnp.float32) + projected).astype(jnp.bfloat16)
    route_weight = group_prob[:, None] * jax.nn.softmax(route_logits, axis=-1)
    most_rows = N_SP * CAP

    def one_expert(carry, inputs):
        index, gate_mat, up_mat, down_mat = inputs
        chosen = expert_ids == index
        named = jnp.any(chosen, axis=1)
        row_index = jnp.nonzero(named, size=most_rows, fill_value=0)[0].astype(jnp.int32)
        valid = jnp.arange(most_rows) < jnp.sum(named.astype(jnp.int32))
        weight_row = lax.optimization_barrier(jnp.sum(jnp.where(chosen, route_weight, 0.0), axis=1))
        rows = jnp.take(mixed, row_index, axis=0)
        gate_part = jnp.dot(rows, gate_mat, preferred_element_type=jnp.float32)
        up_part = jnp.dot(rows, up_mat, preferred_element_type=jnp.float32)
        hidden = (jax.nn.silu(gate_part) * up_part).astype(jnp.bfloat16)
        expert_out = jnp.dot(hidden, down_mat, preferred_element_type=jnp.float32).astype(jnp.bfloat16)
        scaled = jnp.where(valid, jnp.take(weight_row, row_index), 0.0)
        carry = carry.at[row_index].add(scaled[:, None] * expert_out.astype(jnp.float32))
        return (carry, None)
    routed, _ = lax.scan(one_expert, jnp.zeros((TOKENS, D), jnp.float32), (jnp.arange(EXPERTS, dtype=jnp.int32), w_gate, w_up, w_down))
    return (mixed.astype(jnp.float32) + routed).astype(jnp.bfloat16)
```

```python
import functools

import jax
import jax.numpy as jnp
from jax import lax
from jax.experimental import pallas as pl
from jax.experimental.pallas import tpu as pltpu
from jax.sharding import PartitionSpec as P

MESH = pl.DeviceIdType.MESH


def expert_kernel(
    n_sp,
    n_tp,
    value,
    gate,
    taps,
    gain,
    proj,
    resid,
    ids,
    logits,
    prob,
    w_gate,
    w_up,
    w_down,
    out,
    padded,
    sums,
    halo_out,
    halo_in,
    gains,
    stats,
    flip,
    columns,
    act,
    normal,
    mixed,
    slots,
    total,
    outgoing,
    rows,
    hidden,
    results,
    returned,
    gate_v,
    up_v,
    down_v,
    load_sem,
    own_sem,
    halo_sem,
    gain_send,
    gain_recv,
    stat_send,
    stat_recv,
    head_send,
    head_recv,
    act_recv,
    act_far,
    act_near,
    out_send,
    rows_recv,
    rows_far,
    rows_near,
    hid_recv,
    hid_far,
    hid_near,
    ret_send,
    ret_recv,
):
    e = lax.axis_index("sp")
    q = lax.axis_index("tp")
    n_y = n_tp // 2
    y, core = q // 2, q % 2
    sibling = 2 * y + (1 - core)
    _, capacity, width = results.shape
    tokens = mixed.shape[0]
    ff_local = gate_v.shape[1]
    history, local = halo_in.shape
    taken = taps.shape[0]

    def source(k):
        if n_sp & (n_sp - 1) or n_sp == 1:
            return lax.rem(e + k, n_sp)
        k = jnp.where(k == 0, 0, lax.rem(k, n_sp - 1) + 1) if n_sp > 2 else k
        at, bit = 0, 1
        while bit < n_sp:
            at, bit = at + (e // bit + k // bit) % 2 * bit, 2 * bit
        return at

    def target(k):
        if n_sp & (n_sp - 1) or n_sp == 1:
            return lax.rem(e + n_sp - k, n_sp)
        return source(k)

    def rows_at(s, t):
        return rows.at[s, :, pl.ds(pl.multiple_of(t * width, width), width)]

    def act_at(s, t):
        return act.at[t, pl.ds(history, tokens - history)]

    def head_at(t):
        return act.at[t, pl.ds(0, history)]

    def hidden_at(s, t):
        return hidden.at[s, :, pl.ds(pl.multiple_of(t * ff_local, ff_local), ff_local)]

    def far(j):
        return 2 * lax.rem(y + j, n_y) + core

    def behind(j):
        return 2 * lax.rem(y + n_y - j, n_y) + core

    def share(at, recv, s, t, send, peer):
        return pltpu.make_async_remote_copy(
            src_ref=at(s, t),
            dst_ref=at(s, t),
            send_sem=send,
            recv_sem=recv.at[s, t],
            device_id=(e, peer),
            device_id_type=MESH,
        )

    def dispatch(k):
        to = target(k)
        return pltpu.make_async_remote_copy(
            src_ref=outgoing.at[to],
            dst_ref=rows_at(e, q),
            send_sem=out_send.at[k],
            recv_sem=rows_recv.at[e, q],
            device_id=(to, q),
            device_id_type=MESH,
        )

    def give_back(k):
        s = source(k)
        return pltpu.make_async_remote_copy(
            src_ref=results.at[s],
            dst_ref=returned.at[e],
            send_sem=ret_send.at[k],
            recv_sem=ret_recv.at[e],
            device_id=(s, q),
            device_id_type=MESH,
        )

    def arrived(at, recv, s, t):
        pltpu.make_async_copy(at(s, t), at(s, t), recv.at[s, t]).wait()

    def tell(o, source, target, send, recv):
        return pltpu.make_async_remote_copy(
            src_ref=source,
            dst_ref=target,
            send_sem=send.at[o],
            recv_sem=recv.at[q],
            device_id=(e, lax.rem(q + o, n_tp)),
            device_id_type=MESH,
        )

    def tell_gain(o):
        return tell(o, gain, gains.at[q], gain_send, gain_recv)

    def tell_stats(o):
        return tell(o, stats.at[q], stats.at[q], stat_send, stat_recv)

    def tell_head(o):
        return tell(o, head_at(q), head_at(q), head_send, head_recv)

    def heard(ref, recv, t):
        pltpu.make_async_copy(ref, ref, recv.at[t]).wait()

    def hand_on():
        return pltpu.make_async_remote_copy(
            src_ref=halo_out,
            dst_ref=halo_in,
            send_sem=halo_sem.at[0],
            recv_sem=halo_sem.at[1],
            device_id=(lax.rem(e + 1, n_sp), q),
            device_id_type=MESH,
        )

    loads = [
        pltpu.make_async_copy(w_gate.at[0], gate_v, load_sem.at[0]),
        pltpu.make_async_copy(w_up.at[0], up_v, load_sem.at[1]),
        pltpu.make_async_copy(w_down.at[0], down_v, load_sem.at[2]),
    ]
    barrier = pltpu.get_barrier_semaphore()

    @pl.loop(1, n_sp)
    def _(k):
        pl.semaphore_signal(barrier, inc=1, device_id=(source(k), q), device_id_type=MESH)

    for o in range(1, n_tp):
        pl.semaphore_signal(
            barrier, inc=1, device_id=(e, lax.rem(q + o, n_tp)), device_id_type=MESH
        )
    for load in loads:
        load.start()

    flow = value[...].astype(jnp.float32) / (1.0 + jnp.exp(-gate[...].astype(jnp.float32)))
    flow = jnp.transpose(flow).astype(jnp.bfloat16)
    halo_out[...] = flow[tokens - history :]
    padded[history:] = flow.astype(jnp.float32)
    lane = lax.broadcasted_iota(jnp.int32, (history, 128), 1)

    def convolve(first):
        filtered = jnp.zeros((history, local), jnp.float32)
        for j in range(taken):
            at = first + history - (taken - 1) + j
            filtered = filtered + taps[j : j + 1] * padded[at : at + history]
        one = jnp.sum(filtered, axis=1, keepdims=True)
        two = jnp.sum(filtered * filtered, axis=1, keepdims=True)
        sums[first : first + history] = jnp.where(lane == 0, one, jnp.where(lane == 1, two, 0.0))
        act[q, first : first + history] = (filtered - one / local).astype(act.dtype)

    for first in range(history, tokens, history):
        convolve(first)
    gains[q] = gain[...]

    top = ids.shape[0]
    ahead = lax.broadcasted_iota(jnp.int32, (tokens, tokens), 0)
    after = lax.broadcasted_iota(jnp.int32, (tokens, tokens), 1)
    lanes = max(128, n_sp)
    row_no = lax.broadcasted_iota(jnp.int32, (lanes, tokens), 0)
    row_hit = [jnp.where(row_no == ids[r : r + 1], 1.0, 0.0) for r in range(top)]
    row_rank = jnp.dot(
        sum(row_hit).astype(jnp.bfloat16),
        jnp.where(ahead < after, 1.0, 0.0).astype(jnp.bfloat16),
        preferred_element_type=jnp.float32,
    )
    slot_rows = [
        (ids[r : r + 1] * capacity).astype(jnp.float32)
        + jnp.sum(row_hit[r] * row_rank, axis=0, keepdims=True)
        for r in range(top)
    ]
    scores = logits[...]
    scores = jnp.exp(scores - jnp.max(scores, axis=0, keepdims=True))
    scores = prob[...] * scores / jnp.sum(scores, axis=0, keepdims=True)
    flip[...] = jnp.zeros_like(flip)
    for r in range(top):
        flip[r : r + 1] = slot_rows[r]
    flip[top : 2 * top] = scores
    slots[...] = jnp.transpose(flip[...])

    pl.semaphore_wait(barrier, n_sp - 1 + n_tp - 1)

    def spread(at, recv, far_sem, near_sem, s):
        for j in range(1, n_y):
            share(at, recv, s, q, far_sem.at[s, j], far(j)).start()
        share(at, recv, s, q, near_sem.at[s, 0], sibling).start()

    def relay(at, recv, near_sem, s):
        for j in range(1, n_y):
            t = behind(j)
            arrived(at, recv, s, t)
            share(at, recv, s, t, near_sem.at[s, j], sibling).start()

    def collect(at, recv, s):
        for j in range(n_y):
            arrived(at, recv, s, 2 * lax.rem(y + n_y - j, n_y) + (1 - core))

    def drain(at, recv, far_sem, near_sem, s):
        for j in range(1, n_y):
            share(at, recv, s, q, far_sem.at[s, j], far(j)).wait_send()
        share(at, recv, s, q, near_sem.at[s, 0], sibling).wait_send()
        for j in range(1, n_y):
            share(at, recv, s, behind(j), near_sem.at[s, j], sibling).wait_send()

    @pl.when(e + 1 < n_sp)
    def _():
        hand_on().start()

    for j in range(1, n_y):
        share(act_at, act_recv, 0, q, act_far.at[0, j], far(j)).start()
    share(act_at, act_recv, 0, q, act_near.at[0, 0], sibling).start()
    for o in range(1, n_tp):
        tell_gain(o).start()

    @pl.when(e > 0)
    def _():
        hand_on().wait_recv()
        padded[0:history] = halo_in[...].astype(jnp.float32)

    @pl.when(e == 0)
    def _():
        padded[0:history] = jnp.zeros_like(halo_in).astype(jnp.float32)

    convolve(0)
    stats[q] = jnp.transpose(sums[...])[0:8]
    for o in range(1, n_tp):
        tell_head(o).start()
        tell_stats(o).start()
    relay(act_at, act_recv, act_near, 0)
    for o in range(1, n_tp):
        t = lax.rem(q + o, n_tp)
        heard(stats.at[t], stat_recv, t)
        heard(gains.at[t], gain_recv, t)
    channels = proj.shape[0]
    one = stats[0, 0:1]
    two = stats[0, 1:2]
    for t in range(1, n_tp):
        one = one + stats[t, 0:1]
        two = two + stats[t, 1:2]
    mean = one / channels
    scale = lax.rsqrt(two / channels - mean * mean + 1e-05)
    for t in range(n_tp):
        flip[t : t + 1] = (stats[t, 0:1] / local - mean) * scale
    flip[n_tp : n_tp + 1] = scale
    columns[...] = jnp.transpose(flip[...])
    for o in range(1, n_tp):
        t = lax.rem(q + o, n_tp)
        heard(head_at(t), head_recv, t)
    collect(act_at, act_recv, 0)
    step = min(64, tokens)
    for first in range(0, tokens, step):
        for t in range(n_tp):
            scaled = act[t, first : first + step].astype(jnp.float32)
            scaled = scaled * columns[first : first + step, n_tp : n_tp + 1]
            scaled = (scaled + columns[first : first + step, t : t + 1]) * gains[t]
            scaled = scaled / (1.0 + jnp.exp(-scaled))
            normal[first : first + step, t * local : (t + 1) * local] = scaled.astype(normal.dtype)
    mixed[...] = (
        resid[...].astype(jnp.float32)
        + jnp.dot(normal[...], proj[...], preferred_element_type=jnp.float32)
    ).astype(mixed.dtype)

    @pl.loop(0, n_sp)
    def _(k):
        to = target(k)
        place = (to * capacity + lax.broadcasted_iota(jnp.int32, (capacity, tokens), 0)).astype(
            jnp.float32
        )
        picks = jnp.zeros((capacity, tokens), jnp.float32)
        for r in range(top):
            picks = picks + jnp.where(place == slot_rows[r], 1.0, 0.0)
        outgoing[to] = jnp.dot(
            picks.astype(mixed.dtype), mixed[...], preferred_element_type=jnp.float32
        ).astype(outgoing.dtype)

        @pl.when(k > 0)
        def _():
            dispatch(k).start()

    total[...] = jnp.zeros_like(total)
    own_in = pltpu.make_async_copy(outgoing.at[e], rows_at(e, q), own_sem.at[0])
    own_in.start()

    def combine(x):
        place = (x * capacity + lax.broadcasted_iota(jnp.int32, (tokens, capacity), 1)).astype(
            jnp.float32
        )
        for r in range(top):
            picks = jnp.where(place == slots[:, r : r + 1], 1.0, 0.0).astype(mixed.dtype)
            got = jnp.dot(picks, returned[x], preferred_element_type=jnp.float32)
            total[...] += slots[:, top + r : top + r + 1] * got

    tile = min(256, ff_local)
    out_tile = min(256, width)

    def up_step(s):
        @pl.loop(0, ff_local // tile)
        def _(i):
            at = pl.ds(pl.multiple_of(i * tile, tile), tile)
            g = jnp.dot(rows[s], gate_v[:, at], preferred_element_type=jnp.float32)
            u = jnp.dot(rows[s], up_v[:, at], preferred_element_type=jnp.float32)
            h = (g / (1.0 + jnp.exp(-g)) * u).astype(hidden.dtype)
            hidden[s, :, pl.ds(pl.multiple_of(q * ff_local + i * tile, tile), tile)] = h

    def down_step(s):
        @pl.loop(0, width // out_tile)
        def _(i):
            at = pl.ds(pl.multiple_of(i * out_tile, out_tile), out_tile)
            o = jnp.dot(hidden[s], down_v[:, at], preferred_element_type=jnp.float32)
            results[s, :, at] = o.astype(results.dtype)

    @pl.loop(0, n_sp + 4)
    def _(i):
        @pl.when(i < n_sp)
        def _():
            @pl.when(i == 0)
            def _():
                own_in.wait()

            @pl.when(i > 0)
            def _():
                arrived(rows_at, rows_recv, source(i), q)

            spread(rows_at, rows_recv, rows_far, rows_near, source(i))

        @pl.when((i >= 1) & (i < n_sp + 1))
        def _():
            relay(rows_at, rows_recv, rows_near, source(i - 1))

        @pl.when((i >= 2) & (i < n_sp + 2))
        def _():
            s = source(i - 2)
            collect(rows_at, rows_recv, s)

            @pl.when(i == 2)
            def _():
                for load in loads:
                    load.wait()

            up_step(s)
            spread(hidden_at, hid_recv, hid_far, hid_near, s)

        @pl.when((i >= 3) & (i < n_sp + 3))
        def _():
            relay(hidden_at, hid_recv, hid_near, source(i - 3))

        @pl.when(i >= 4)
        def _():
            s = source(i - 4)
            collect(hidden_at, hid_recv, s)
            down_step(s)

            @pl.when(i == 4)
            def _():
                pltpu.make_async_copy(results.at[e], returned.at[e], own_sem.at[1]).start()

            @pl.when(i > 4)
            def _():
                give_back(i - 4).start()

    pltpu.make_async_copy(results.at[e], returned.at[e], own_sem.at[1]).wait()
    combine(e)

    @pl.loop(1, n_sp)
    def _(k):
        x = target(k)
        pltpu.make_async_copy(returned.at[x], returned.at[x], ret_recv.at[x]).wait()
        combine(x)

    out[...] = (mixed[...].astype(jnp.float32) + total[...]).astype(out.dtype)

    @pl.when(e + 1 < n_sp)
    def _():
        hand_on().wait_send()

    for o in range(1, n_tp):
        tell_gain(o).wait_send()
        tell_head(o).wait_send()
        tell_stats(o).wait_send()
    drain(act_at, act_recv, act_far, act_near, 0)

    @pl.loop(0, n_sp)
    def _(s):
        drain(rows_at, rows_recv, rows_far, rows_near, s)
        drain(hidden_at, hid_recv, hid_far, hid_near, s)

    @pl.loop(1, n_sp)
    def _(k):
        dispatch(k).wait_send()
        give_back(k).wait_send()


def run_layer(value, gate, taps, gain, proj, resid, ids, logits, prob, w_gate, w_up, w_down):
    n_sp, n_tp = lax.axis_size("sp"), lax.axis_size("tp")
    n_y = n_tp // 2
    tokens, width = resid.shape
    local = value.shape[0]
    capacity = 4 * tokens // n_sp
    ff_local = w_gate.shape[2]
    history = -(-(taps.shape[0] - 1) // 16) * 16
    dma = pltpu.SemaphoreType.DMA
    vmem = pl.BlockSpec(memory_space=pltpu.VMEM)
    return pl.pallas_call(
        functools.partial(expert_kernel, n_sp, n_tp),
        out_shape=jax.ShapeDtypeStruct(resid.shape, resid.dtype),
        in_specs=[vmem] * 9 + [pl.BlockSpec(memory_space=pl.ANY)] * 3,
        out_specs=vmem,
        scratch_shapes=[
            pltpu.VMEM((history + tokens, local), jnp.float32),
            pltpu.VMEM((tokens, 128), jnp.float32),
            pltpu.VMEM((history, local), jnp.bfloat16),
            pltpu.VMEM((history, local), jnp.bfloat16),
            pltpu.VMEM((n_tp, 1, local), jnp.float32),
            pltpu.VMEM((n_tp, 8, tokens), jnp.float32),
            pltpu.VMEM((128, tokens), jnp.float32),
            pltpu.VMEM((tokens, 128), jnp.float32),
            pltpu.VMEM((n_tp, tokens, local), jnp.bfloat16),
            pltpu.VMEM((tokens, local * n_tp), jnp.bfloat16),
            pltpu.VMEM((tokens, width), jnp.bfloat16),
            pltpu.VMEM((tokens, 128), jnp.float32),
            pltpu.VMEM((tokens, width), jnp.float32),
            pltpu.VMEM((n_sp, capacity, width), jnp.bfloat16),
            pltpu.VMEM((n_sp, capacity, width * n_tp), jnp.bfloat16),
            pltpu.VMEM((n_sp, capacity, ff_local * n_tp), jnp.bfloat16),
            pltpu.VMEM((n_sp, capacity, width), jnp.bfloat16),
            pltpu.VMEM((n_sp, capacity, width), jnp.bfloat16),
            pltpu.VMEM(w_gate.shape[1:], jnp.bfloat16),
            pltpu.VMEM(w_up.shape[1:], jnp.bfloat16),
            pltpu.VMEM(w_down.shape[1:], jnp.bfloat16),
            dma((3,)),
            dma((2,)),
            dma((2,)),
            dma((n_tp,)),
            dma((n_tp,)),
            dma((n_tp,)),
            dma((n_tp,)),
            dma((n_tp,)),
            dma((n_tp,)),
            dma((1, n_tp)),
            dma((1, n_y)),
            dma((1, n_y)),
            dma((n_sp,)),
            dma((n_sp, n_tp)),
            dma((n_sp, n_y)),
            dma((n_sp, n_y)),
            dma((n_sp, n_tp)),
            dma((n_sp, n_y)),
            dma((n_sp, n_y)),
            dma((n_sp,)),
            dma((n_sp,)),
        ],
        compiler_params=pltpu.CompilerParams(
            collective_id=0, has_side_effects=True, vmem_limit_bytes=52 * 1024 * 1024
        ),
    )(value, gate, taps, gain, proj, resid, ids, logits, prob, w_gate, w_up, w_down)


def per_device(
    glu_value,
    glu_gate,
    conv_taps,
    norm_gain,
    out_proj,
    resid,
    expert_ids,
    route_logits,
    group_prob,
    w_gate,
    w_up,
    w_down,
):
    return run_layer(
        glu_value,
        glu_gate,
        conv_taps.T,
        norm_gain[None, :],
        out_proj,
        resid,
        expert_ids.T,
        route_logits.T,
        group_prob[None, :],
        w_gate,
        w_up,
        w_down,
    )


def solution(mesh):
    return jax.shard_map(
        per_device,
        mesh=mesh,
        in_specs=(
            P("tp", "sp"),
            P("tp", "sp"),
            P("tp", None),
            P("tp"),
            P(None, "tp"),
            P("sp", "tp"),
            P("sp", None),
            P("sp", None),
            P("sp"),
            P("sp", None, "tp"),
            P("sp", None, "tp"),
            P("sp", None, "tp"),
        ),
        out_specs=P("sp", "tp"),
        check_vma=False,
    )
```

```python
import functools

import jax
import jax.numpy as jnp
from jax import lax
from jax.experimental import pallas as pl
from jax.experimental.pallas import tpu as pltpu
from jax.sharding import PartitionSpec as P

MESH = pl.DeviceIdType.MESH


def expert_kernel(
    n_sp,
    n_tp,
    front,
    value_h,
    gate_h,
    taps_h,
    gain_h,
    proj_h,
    resid_h,
    ids_h,
    logits_h,
    prob_h,
    w_gate,
    w_up,
    w_down,
    out,
    value,
    gate,
    taps,
    gain,
    proj,
    resid,
    ids,
    logits,
    prob,
    padded,
    sums,
    halo_out,
    halo_in,
    gains,
    stats,
    stats_head,
    flip,
    columns,
    flip_head,
    columns_head,
    act,
    normal,
    mixed,
    mixed_front,
    picks,
    picks_back,
    weights,
    total,
    outgoing,
    outgoing_front,
    rows,
    hidden,
    results,
    returned,
    gate_v,
    up_v,
    down_v,
    input_sem,
    load_sem,
    halo_sem,
    gain_send,
    gain_recv,
    stat_send,
    stat_recv,
    head_send,
    head_recv,
    last_send,
    last_recv,
    act_recv,
    act_far,
    act_near,
    front_send,
    front_recv,
    whole_send,
    whole_recv,
    part_send,
    part_recv,
    cross_send,
    cross_recv,
    half_send,
    half_recv,
    hid_recv,
    hid_far,
    hid_near,
    ret_send,
    ret_recv,
):
    e = lax.axis_index("sp")
    q = lax.axis_index("tp")
    n_y = n_tp // 2
    y, core = q // 2, q % 2
    sibling = 2 * y + (1 - core)
    _, capacity, width = results.shape
    tokens = mixed.shape[0]
    ff_local = gate_v.shape[1]
    history, local = halo_in.shape
    taken = taps.shape[0]
    top = ids.shape[0]
    middle = history + (tokens - history) // 32 * 16
    pieces = ((history, middle - history), (middle, tokens - middle))
    power = n_sp > 1 and n_sp & (n_sp - 1) == 0
    bits = [e // 2**b % 2 for b in range(n_sp.bit_length() - 1)]

    def source(k):
        if not power:
            return lax.rem(e + k, n_sp)
        if n_sp > 4:
            k = jnp.where(k < 3, lax.rem(2 * k, 3), jnp.where(k == n_sp - 1, 3, k + 1))
        return sum((bits[b] + k // 2**b) % 2 * 2**b for b in range(len(bits)))

    def target(k):
        return source(k) if power else lax.rem(e + n_sp - k, n_sp)

    def far(j):
        return 2 * lax.rem(y + j, n_y) + core

    def above(j):
        return lax.rem(y + j, n_y)

    def below(j):
        return lax.rem(y + n_y - j, n_y)

    def quarter(s, of, first, size):
        at = pl.multiple_of((core * n_y + of) * width + first, min(128, width))
        return rows.at[s, :, pl.ds(at, size)]

    def half(s, c):
        return rows.at[s, :, pl.ds(pl.multiple_of(c * n_y * width, width), n_y * width)]

    def hidden_at(s, t):
        return hidden.at[s, :, pl.ds(pl.multiple_of(t * ff_local, ff_local), ff_local)]

    def remote(src, dst, send, recv, to):
        return pltpu.make_async_remote_copy(
            src_ref=src,
            dst_ref=dst,
            send_sem=send,
            recv_sem=recv,
            device_id=to,
            device_id_type=MESH,
        )

    def arrived(ref, recv):
        pltpu.make_async_copy(ref, ref, recv).wait()

    def tell(o, ref, to, send, recv):
        return remote(ref, to, send.at[o], recv.at[q], (e, lax.rem(q + o, n_tp)))

    def tell_gain(o):
        return tell(o, gain, gains.at[q], gain_send, gain_recv)

    def tell_stats(o):
        return tell(o, stats.at[q], stats.at[q], stat_send, stat_recv)

    def tell_last(o):
        return tell(o, stats_head.at[q], stats_head.at[q], last_send, last_recv)

    def head_at(t):
        return act.at[t, pl.ds(0, history)]

    def tell_head(o):
        return tell(o, head_at(q), head_at(q), head_send, head_recv)

    def hand_on():
        to = (lax.rem(e + 1, n_sp), q)
        return remote(halo_out, halo_in, halo_sem.at[0], halo_sem.at[1], to)

    def piece_at(p, t):
        return act.at[t, pl.ds(pieces[p][0], pieces[p][1])]

    def piece(p, t, send, to):
        return remote(piece_at(p, t), piece_at(p, t), send, act_recv.at[p, t], (e, to))

    def share_front(j):
        ours = mixed.at[:, pl.ds(0, front)]
        return remote(ours, mixed_front.at[y], front_send.at[j], front_recv.at[y], (e, far(j)))

    def dispatch(k):
        to = target(k)
        return remote(
            outgoing.at[to],
            quarter(e, y, 0, width),
            whole_send.at[k],
            whole_recv.at[e],
            (to, q),
        )

    def dispatch_front(k, j):
        to = target(k)
        return remote(
            outgoing_front.at[j - 1, to],
            quarter(e, above(j), 0, front),
            part_send.at[k, j],
            part_recv.at[e, above(j)],
            (to, q),
        )

    def cross(s, j, first):
        ref = quarter(s, y, first, width - first)
        return remote(ref, ref, cross_send.at[s, j], cross_recv.at[s, y], (e, far(j)))

    def halve(s):
        ref = half(s, core)
        return remote(ref, ref, half_send.at[s], half_recv.at[s], (e, sibling))

    def share(s, t, send, to):
        ref = hidden_at(s, t)
        return remote(ref, ref, send, hid_recv.at[s, t], (e, to))

    def give_back(k):
        s = source(k)
        return remote(
            results.at[s], returned.at[e], ret_send.at[k], ret_recv.at[e], (s, q)
        )

    inputs = [
        pltpu.make_async_copy(there, here, input_sem.at[i])
        for i, (there, here) in enumerate(
            (
                (value_h, value),
                (gate_h, gate),
                (taps_h, taps),
                (ids_h, ids),
                (logits_h, logits),
                (prob_h, prob),
                (gain_h, gain),
                (proj_h, proj),
                (resid_h, resid),
            )
        )
    ]
    loads = []
    for i, (there, here) in enumerate(((w_gate, gate_v), (w_up, up_v))):
        for t in range(n_tp):
            at = (t % 2 * n_y + t // 2) * width
            loads.append(
                pltpu.make_async_copy(
                    there.at[0, pl.ds(t * width, width)],
                    here.at[pl.ds(at, width)],
                    load_sem.at[i * n_tp + t],
                )
            )
    loads.append(pltpu.make_async_copy(w_down.at[0], down_v, load_sem.at[2 * n_tp]))
    for copy in inputs:
        copy.start()
    barrier = pltpu.get_barrier_semaphore()

    @pl.loop(1, n_sp)
    def _(k):
        pl.semaphore_signal(barrier, inc=1, device_id=(source(k), q), device_id_type=MESH)

    for o in range(1, n_tp):
        pl.semaphore_signal(
            barrier, inc=1, device_id=(e, lax.rem(q + o, n_tp)), device_id_type=MESH
        )
    for copy in inputs[:3]:
        copy.wait()
    for load in loads:
        load.start()

    flow = value[...].astype(jnp.float32) / (1.0 + jnp.exp(-gate[...].astype(jnp.float32)))
    flow = jnp.transpose(flow).astype(jnp.bfloat16)
    halo_out[...] = flow[tokens - history :]
    padded[history:] = flow.astype(jnp.float32)
    lane = lax.broadcasted_iota(jnp.int32, (history, 128), 1)

    def convolve(first):
        filtered = jnp.zeros((history, local), jnp.float32)
        for j in range(taken):
            at = first + history - (taken - 1) + j
            filtered = filtered + taps[j : j + 1] * padded[at : at + history]
        one = jnp.sum(filtered, axis=1, keepdims=True)
        two = jnp.sum(filtered * filtered, axis=1, keepdims=True)
        sums[first : first + history] = jnp.where(lane == 0, one, jnp.where(lane == 1, two, 0.0))
        act[q, first : first + history] = (filtered - one / local).astype(act.dtype)

    sums[0:history] = jnp.zeros((history, 128), jnp.float32)
    for first in range(history, tokens, history):
        convolve(first)
    stats[q] = jnp.transpose(sums[...])[0:8]
    for copy in inputs[3:]:
        copy.wait()
    gains[q] = gain[...]
    pl.semaphore_wait(barrier, n_sp - 1 + n_tp - 1)

    @pl.when(e + 1 < n_sp)
    def _():
        hand_on().start()

    for o in range(1, n_tp):
        tell_gain(o).start()
        tell_stats(o).start()
    for p in range(2):
        for j in range(1, n_y):
            piece(p, q, act_far.at[p, j], far(j)).start()
        piece(p, q, act_near.at[p, 0], sibling).start()

    ahead = lax.broadcasted_iota(jnp.int32, (tokens, tokens), 0)
    after = lax.broadcasted_iota(jnp.int32, (tokens, tokens), 1)
    lanes = max(128, n_sp)
    row_no = lax.broadcasted_iota(jnp.int32, (lanes, tokens), 0)
    row_hit = [jnp.where(row_no == ids[r : r + 1], 1.0, 0.0) for r in range(top)]
    row_rank = jnp.dot(
        sum(row_hit).astype(jnp.bfloat16),
        jnp.where(ahead < after, 1.0, 0.0).astype(jnp.bfloat16),
        preferred_element_type=jnp.float32,
    )
    slot_rows = [
        (ids[r : r + 1] * capacity).astype(jnp.float32)
        + jnp.sum(row_hit[r] * row_rank, axis=0, keepdims=True)
        for r in range(top)
    ]
    scores = logits[...]
    scores = jnp.exp(scores - jnp.max(scores, axis=0, keepdims=True))
    scores = prob[...] * scores / jnp.sum(scores, axis=0, keepdims=True)
    weights[...] = jnp.transpose(sum(row_hit[r] * scores[r : r + 1] for r in range(top)))

    @pl.when(e > 0)
    def _():
        hand_on().wait_recv()
        padded[0:history] = halo_in[...].astype(jnp.float32)

    @pl.when(e == 0)
    def _():
        padded[0:history] = jnp.zeros_like(halo_in).astype(jnp.float32)

    convolve(0)
    stats_head[q] = jnp.transpose(jnp.concatenate([sums[0:history]] * (128 // history), axis=0))[0:8]
    for o in range(1, n_tp):
        tell_head(o).start()
        tell_last(o).start()

    @pl.loop(0, n_sp)
    def _(x):
        place = (x * capacity + lax.broadcasted_iota(jnp.int32, (capacity, tokens), 0)).astype(
            jnp.float32
        )
        chosen = jnp.zeros((capacity, tokens), jnp.float32)
        for r in range(top):
            chosen = chosen + jnp.where(place == slot_rows[r], 1.0, 0.0)
        picks[x] = chosen.astype(picks.dtype)
        picks_back[x] = jnp.transpose(chosen).astype(picks.dtype)

    total[...] = jnp.zeros_like(total)
    channels = proj.shape[0]

    def moments(table, into, turned):
        one = table[0, 0:1]
        two = table[0, 1:2]
        for t in range(1, n_tp):
            one = one + table[t, 0:1]
            two = two + table[t, 1:2]
        mean = one / channels
        scale = lax.rsqrt(two / channels - mean * mean + 1e-05)
        into[...] = jnp.zeros_like(into)
        for t in range(n_tp):
            into[t : t + 1] = (table[t, 0:1] / local - mean) * scale
        into[n_tp : n_tp + 1] = scale
        turned[...] = jnp.transpose(into[...])

    def norm(first, size, turned):
        for t in range(n_tp):
            scaled = act[t, first : first + size].astype(jnp.float32)
            scaled = scaled * turned[first : first + size, n_tp : n_tp + 1]
            scaled = (scaled + turned[first : first + size, t : t + 1]) * gains[t]
            scaled = scaled / (1.0 + jnp.exp(-scaled))
            normal[first : first + size, t * local : (t + 1) * local] = scaled.astype(normal.dtype)

    for o in range(1, n_tp):
        t = lax.rem(q + o, n_tp)
        arrived(stats.at[t], stat_recv.at[t])
        arrived(gains.at[t], gain_recv.at[t])
    moments(stats, flip, columns)
    for p in range(2):
        for j in range(1, n_y):
            t = 2 * below(j) + core
            arrived(piece_at(p, t), act_recv.at[p, t])
            piece(p, t, act_near.at[p, j], sibling).start()
    for p in range(2):
        for j in range(n_y):
            t = 2 * below(j) + (1 - core)
            arrived(piece_at(p, t), act_recv.at[p, t])
        first, size = pieces[p]
        step = 56 if size % 56 == 0 else 16
        for at in range(first, first + size, step):
            norm(at, step, columns)
    for o in range(1, n_tp):
        t = lax.rem(q + o, n_tp)
        arrived(stats_head.at[t], last_recv.at[t])
        arrived(head_at(t), head_recv.at[t])
    moments(stats_head, flip_head, columns_head)
    norm(0, history, columns_head)
    mixed[...] = (
        resid[...].astype(jnp.float32)
        + jnp.dot(normal[...], proj[...], preferred_element_type=jnp.float32)
    ).astype(mixed.dtype)

    def pick(x, block):
        got = jnp.dot(picks[x], block, preferred_element_type=jnp.float32)
        return got.astype(outgoing.dtype)

    quarter(e, y, 0, width)[...] = pick(e, mixed[...])
    for j in range(1, n_y):
        cross(e, j, 0).start()
    if front:
        for j in range(1, n_y):
            share_front(j).start()
    near = min(3, n_sp - 1)

    def send(k):
        to = target(k)
        outgoing[to] = pick(to, mixed[...])
        dispatch(k).start()

    def send_front(k):
        to = target(k)
        for j in range(1, n_y):
            outgoing_front[j - 1, to] = pick(to, mixed_front[above(j)])
            dispatch_front(k, j).start()

    pl.loop(1, near)(send)

    def begin(k):
        s = source(k)
        arrived(quarter(s, y, 0, width), whole_recv.at[s])
        for first, chosen in ((0, k < near), (front, k >= near)):

            @pl.when(chosen)
            def _():
                for j in range(1, n_y):
                    cross(s, j, first).start()

    def gather(k):
        s = source(k)
        for first, chosen in ((0, k < near), (front, k >= near)):

            @pl.when(chosen)
            def _():
                for j in range(1, n_y):
                    of = below(j)
                    if first:
                        arrived(quarter(s, of, 0, first), part_recv.at[s, of])
                    arrived(quarter(s, of, first, width - first), cross_recv.at[s, of])

        halve(s).start()

    for j in range(1, n_y):
        arrived(quarter(e, below(j), 0, width), cross_recv.at[e, below(j)])
    halve(e).start()
    send(near)
    begin(1)
    for load in loads:
        load.wait()

    tile = min(256, ff_local)
    out_tile = min(256, width)

    def up_step(s):
        @pl.loop(0, ff_local // tile)
        def _(i):
            at = pl.ds(pl.multiple_of(i * tile, tile), tile)
            g = jnp.dot(rows[s], gate_v[:, at], preferred_element_type=jnp.float32)
            u = jnp.dot(rows[s], up_v[:, at], preferred_element_type=jnp.float32)
            h = (g / (1.0 + jnp.exp(-g)) * u).astype(hidden.dtype)
            hidden[s, :, pl.ds(pl.multiple_of(q * ff_local + i * tile, tile), tile)] = h

    def down_step(s):
        @pl.loop(0, width // out_tile)
        def _(i):
            at = pl.ds(pl.multiple_of(i * out_tile, out_tile), out_tile)
            o = jnp.dot(hidden[s], down_v[:, at], preferred_element_type=jnp.float32)
            results[s, :, at] = o.astype(results.dtype)

    slot_lane = lax.broadcasted_iota(jnp.int32, weights.shape, 1)

    def combine(x, block):
        got = jnp.dot(picks_back[x], block, preferred_element_type=jnp.float32)
        weight = jnp.sum(jnp.where(slot_lane == x, weights[...], 0.0), axis=1, keepdims=True)
        total[...] += weight * got

    def take(k):
        x = target(k)
        arrived(returned.at[x], ret_recv.at[x])
        combine(x, returned[x])

    def drain(k):
        s = source(k)
        halve(s).wait_send()
        share(s, q, hid_near.at[s, 0], sibling).wait_send()
        for j in range(1, n_y):
            share(s, q, hid_far.at[s, j], far(j)).wait_send()
            share(s, 2 * below(j) + core, hid_near.at[s, j], sibling).wait_send()

        for first, chosen in ((0, k < near), (front, k >= near)):

            @pl.when(chosen)
            def _():
                for j in range(1, n_y):
                    cross(s, j, first).wait_send()
                    if first:
                        dispatch_front(k, j).wait_send()

        @pl.when(k > 0)
        def _():
            dispatch(k).wait_send()

    @pl.loop(2, n_sp + 4)
    def _(i):
        @pl.when(i < n_sp + 2)
        def _():
            s = source(i - 2)
            arrived(half(s, 1 - core), half_recv.at[s])
            up_step(s)
            for j in range(1, n_y):
                share(s, q, hid_far.at[s, j], far(j)).start()
            share(s, q, hid_near.at[s, 0], sibling).start()

        if front:

            @pl.when(i == 2)
            def _():
                for j in range(1, n_y):
                    arrived(mixed_front.at[below(j)], front_recv.at[below(j)])

            @pl.when(i - 2 + near < n_sp)
            def _():
                send_front(i - 2 + near)

        @pl.when(i - 1 + near < n_sp)
        def _():
            send(i - 1 + near)

        @pl.when(i < n_sp)
        def _():
            begin(i)

        @pl.when(i < n_sp + 1)
        def _():
            gather(i - 1)

        @pl.when((i >= 3) & (i < n_sp + 3))
        def _():
            s = source(i - 3)
            for j in range(1, n_y):
                t = 2 * below(j) + core
                arrived(hidden_at(s, t), hid_recv.at[s, t])
                share(s, t, hid_near.at[s, j], sibling).start()

        @pl.when(i >= 4)
        def _():
            s = source(i - 4)
            for j in range(n_y):
                t = 2 * below(j) + (1 - core)
                arrived(hidden_at(s, t), hid_recv.at[s, t])
            down_step(s)

            @pl.when(i == 4)
            def _():
                combine(e, results[e])

            @pl.when(i > 4)
            def _():
                give_back(i - 4).start()

        @pl.when(i >= 5)
        def _():
            drain(i - 5)

        @pl.when(i >= 8)
        def _():
            take(i - 7)

    for k in range(max(1, n_sp - 3), n_sp):
        take(k)
    out[...] = (mixed[...].astype(jnp.float32) + total[...]).astype(out.dtype)

    drain(n_sp - 1)

    @pl.loop(1, n_sp)
    def _(k):
        give_back(k).wait_send()

    @pl.when(e + 1 < n_sp)
    def _():
        hand_on().wait_send()

    for o in range(1, n_tp):
        tell_gain(o).wait_send()
        tell_stats(o).wait_send()
        tell_head(o).wait_send()
        tell_last(o).wait_send()
    for p in range(2):
        piece(p, q, act_near.at[p, 0], sibling).wait_send()
        for j in range(1, n_y):
            piece(p, q, act_far.at[p, j], far(j)).wait_send()
            piece(p, 2 * below(j) + core, act_near.at[p, j], sibling).wait_send()
    if front:
        for j in range(1, n_y):
            share_front(j).wait_send()


def run_layer(value, gate, taps, gain, proj, resid, ids, logits, prob, w_gate, w_up, w_down):
    n_sp, n_tp = lax.axis_size("sp"), lax.axis_size("tp")
    n_y = n_tp // 2
    tokens, width = resid.shape
    local = value.shape[0]
    capacity = 4 * tokens // n_sp
    ff_local = w_gate.shape[2]
    history = -(-(taps.shape[0] - 1) // 16) * 16
    front = width // 256 * 128
    span = max(front, 128)
    lanes = max(128, n_sp)
    dma = pltpu.SemaphoreType.DMA
    small = (value, gate, taps, gain, proj, resid, ids, logits, prob)
    return pl.pallas_call(
        functools.partial(expert_kernel, n_sp, n_tp, front),
        out_shape=pltpu.VMEM(resid.shape, resid.dtype),
        in_specs=[pl.BlockSpec(memory_space=pltpu.HBM)] * 12,
        out_specs=pl.BlockSpec(memory_space=pltpu.VMEM),
        scratch_shapes=[pltpu.VMEM(x.shape, x.dtype) for x in small]
        + [
            pltpu.VMEM((history + tokens, local), jnp.float32),
            pltpu.VMEM((tokens, 128), jnp.float32),
            pltpu.VMEM((history, local), jnp.bfloat16),
            pltpu.VMEM((history, local), jnp.bfloat16),
            pltpu.VMEM((n_tp, 1, local), jnp.float32),
            pltpu.VMEM((n_tp, 8, tokens), jnp.float32),
            pltpu.VMEM((n_tp, 8, 128), jnp.float32),
            pltpu.VMEM((128, tokens), jnp.float32),
            pltpu.VMEM((tokens, 128), jnp.float32),
            pltpu.VMEM((128, 128), jnp.float32),
            pltpu.VMEM((128, 128), jnp.float32),
            pltpu.VMEM((n_tp, tokens, local), jnp.bfloat16),
            pltpu.VMEM((tokens, local * n_tp), jnp.bfloat16),
            pltpu.VMEM((tokens, width), jnp.bfloat16),
            pltpu.VMEM((n_y, tokens, span), jnp.bfloat16),
            pltpu.VMEM((n_sp, capacity, tokens), jnp.bfloat16),
            pltpu.VMEM((n_sp, tokens, capacity), jnp.bfloat16),
            pltpu.VMEM((tokens, lanes), jnp.float32),
            pltpu.VMEM((tokens, width), jnp.float32),
            pltpu.VMEM((n_sp, capacity, width), jnp.bfloat16),
            pltpu.VMEM((n_y - 1 if front else 1, n_sp, capacity, span), jnp.bfloat16),
            pltpu.VMEM((n_sp, capacity, width * n_tp), jnp.bfloat16),
            pltpu.VMEM((n_sp, capacity, ff_local * n_tp), jnp.bfloat16),
            pltpu.VMEM((n_sp, capacity, width), jnp.bfloat16),
            pltpu.VMEM((n_sp, capacity, width), jnp.bfloat16),
            pltpu.VMEM(w_gate.shape[1:], jnp.bfloat16),
            pltpu.VMEM(w_up.shape[1:], jnp.bfloat16),
            pltpu.VMEM(w_down.shape[1:], jnp.bfloat16),
            dma((len(small),)),
            dma((2 * n_tp + 1,)),
            dma((2,)),
        ]
        + [dma((n_tp,))] * 8
        + [
            dma((2, n_tp)),
            dma((2, n_y)),
            dma((2, n_y)),
            dma((n_y,)),
            dma((n_y,)),
            dma((n_sp,)),
            dma((n_sp,)),
            dma((n_sp, n_y)),
            dma((n_sp, n_y)),
            dma((n_sp, n_y)),
            dma((n_sp, n_y)),
            dma((n_sp,)),
            dma((n_sp,)),
            dma((n_sp, n_tp)),
            dma((n_sp, n_y)),
            dma((n_sp, n_y)),
            dma((n_sp,)),
            dma((n_sp,)),
        ],
        compiler_params=pltpu.CompilerParams(
            collective_id=0, has_side_effects=True, vmem_limit_bytes=57000000
        ),
    )(*small, w_gate, w_up, w_down)


def per_device(
    glu_value,
    glu_gate,
    conv_taps,
    norm_gain,
    out_proj,
    resid,
    expert_ids,
    route_logits,
    group_prob,
    w_gate,
    w_up,
    w_down,
):
    return run_layer(
        glu_value,
        glu_gate,
        conv_taps.T,
        norm_gain[None, :],
        out_proj,
        resid,
        expert_ids.T,
        route_logits.T,
        group_prob[None, :],
        w_gate,
        w_up,
        w_down,
    )


def solution(mesh):
    return jax.shard_map(
        per_device,
        mesh=mesh,
        in_specs=(
            P("tp", "sp"),
            P("tp", "sp"),
            P("tp", None),
            P("tp"),
            P(None, "tp"),
            P("sp", "tp"),
            P("sp", None),
            P("sp", None),
            P("sp"),
            P("sp", None, "tp"),
            P("sp", None, "tp"),
            P("sp", None, "tp"),
        ),
        out_specs=P("sp", "tp"),
        check_vma=False,
    )
```

```python
import functools

import jax
import jax.numpy as jnp
from jax import lax
from jax.experimental import pallas as pl
from jax.experimental.pallas import tpu as pltpu
from jax.sharding import PartitionSpec as P

MESH = pl.DeviceIdType.MESH


def expert_kernel(
    n_sp,
    n_tp,
    front,
    value_h,
    gate_h,
    taps_h,
    gain_h,
    proj_h,
    resid_h,
    ids_h,
    logits_h,
    prob_h,
    w_gate,
    w_up,
    w_down,
    out,
    value,
    gate,
    taps,
    gain,
    proj,
    resid,
    ids,
    logits,
    prob,
    padded,
    sums,
    halo_out,
    halo_in,
    gains,
    stats,
    stats_head,
    flip,
    columns,
    flip_head,
    columns_head,
    act,
    normal,
    mixed,
    mixed_front,
    slots,
    slots_far,
    tok,
    tok_front,
    picks,
    picks_far,
    picks_back,
    weights,
    total,
    outgoing,
    outgoing_front,
    rows,
    hidden,
    results,
    returned,
    gate_v,
    up_v,
    down_v,
    input_sem,
    load_sem,
    halo_sem,
    gain_send,
    gain_recv,
    stat_send,
    stat_recv,
    head_send,
    head_recv,
    last_send,
    last_recv,
    act_recv,
    act_far,
    act_near,
    front_send,
    front_recv,
    slot_sem,
    tok_sem,
    tok_send,
    tok_recv,
    whole_send,
    whole_recv,
    part_send,
    part_recv,
    cross_send,
    cross_recv,
    half_send,
    half_recv,
    hid_recv,
    hid_far,
    hid_near,
    ret_send,
    ret_recv,
):
    e = lax.axis_index("sp")
    q = lax.axis_index("tp")
    n_y = n_tp // 2
    y, core = q // 2, q % 2
    sibling = 2 * y + (1 - core)
    _, capacity, width = results.shape
    tokens = mixed.shape[0]
    ff_local = gate_v.shape[1]
    parts = hid_recv.shape[2]
    ff_part = ff_local // parts
    history, local = halo_in.shape
    taken = taps.shape[0]
    top = ids.shape[0]
    middle = history + (tokens - history) // 32 * 16
    pieces = ((history, middle - history), (middle, tokens - middle))
    far_by = n_sp // 2
    bits = [e // 2**b % 2 for b in range(n_sp.bit_length() - 1)]

    def moved(v):
        return sum((bits[b] + v // 2**b) % 2 * 2**b for b in range(len(bits)))

    def order(k):
        return lax.rem(k + 1, n_sp)

    def source(k):
        return moved(order(k))

    partner = moved(far_by)

    def far(j):
        return 2 * lax.rem(y + j, n_y) + core

    def above(j):
        return lax.rem(y + j, n_y)

    def below(j):
        return lax.rem(y + n_y - j, n_y)

    def quarter(s, of, first, size):
        at = pl.multiple_of((core * n_y + of) * width + first, min(128, width))
        return rows.at[s, :, pl.ds(at, size)]

    def half(s, c):
        return rows.at[s, :, pl.ds(pl.multiple_of(c * n_y * width, width), n_y * width)]

    def hidden_at(s, t, part):
        at = pl.multiple_of(t * ff_local + part * ff_part, ff_part)
        return hidden.at[s, :, pl.ds(at, ff_part)]

    def remote(src, dst, send, recv, to):
        return pltpu.make_async_remote_copy(
            src_ref=src,
            dst_ref=dst,
            send_sem=send,
            recv_sem=recv,
            device_id=to,
            device_id_type=MESH,
        )

    def arrived(ref, recv):
        pltpu.make_async_copy(ref, ref, recv).wait()

    def tell(o, ref, to, send, recv):
        return remote(ref, to, send.at[o], recv.at[q], (e, lax.rem(q + o, n_tp)))

    def tell_gain(o):
        return tell(o, gain, gains.at[q], gain_send, gain_recv)

    def tell_stats(o):
        return tell(o, stats.at[q], stats.at[q], stat_send, stat_recv)

    def tell_last(o):
        return tell(o, stats_head.at[q], stats_head.at[q], last_send, last_recv)

    def head_at(t):
        return act.at[t, pl.ds(0, history)]

    def tell_head(o):
        return tell(o, head_at(q), head_at(q), head_send, head_recv)

    def hand_on():
        to = (lax.rem(e + 1, n_sp), q)
        return remote(halo_out, halo_in, halo_sem.at[0], halo_sem.at[1], to)

    def piece_at(p, t):
        return act.at[t, pl.ds(pieces[p][0], pieces[p][1])]

    def piece(p, t, send, to):
        return remote(piece_at(p, t), piece_at(p, t), send, act_recv.at[p, t], (e, to))

    def share_front(j):
        ours = mixed.at[:, pl.ds(0, front)]
        return remote(ours, mixed_front.at[y], front_send.at[j], front_recv.at[y], (e, far(j)))

    def share_slots():
        return remote(slots, slots_far, slot_sem.at[0], slot_sem.at[1], (partner, q))

    def share_tokens():
        return remote(mixed, tok, tok_sem.at[0], tok_sem.at[1], (partner, q))

    def share_tokens_front(j):
        of = above(j)
        ours = mixed_front.at[of]
        return remote(ours, tok_front.at[of], tok_send.at[of], tok_recv.at[of], (partner, q))

    def dispatch(v, s):
        to = moved(lax.rem(v, far_by))
        return remote(
            outgoing.at[v], quarter(s, y, 0, width), whole_send.at[v], whole_recv.at[s], (to, q)
        )

    def dispatch_front(v, s, j):
        to = moved(lax.rem(v, far_by))
        of = above(j)
        return remote(
            outgoing_front.at[j - 1, v],
            quarter(s, of, 0, front),
            part_send.at[v, j],
            part_recv.at[s, of],
            (to, q),
        )

    def cross(s, j, first):
        ref = quarter(s, y, first, width - first)
        return remote(ref, ref, cross_send.at[s, j], cross_recv.at[s, y], (e, far(j)))

    def halve(s):
        ref = half(s, core)
        return remote(ref, ref, half_send.at[s], half_recv.at[s], (e, sibling))

    def share(s, part, j):
        ref = hidden_at(s, q, part)
        to = sibling if j == 0 else far(j)
        send = hid_near.at[s, 0, part] if j == 0 else hid_far.at[s, j, part]
        return remote(ref, ref, send, hid_recv.at[s, q, part], (e, to))

    def pass_on(s, part, j):
        t = 2 * below(j) + core
        ref = hidden_at(s, t, part)
        return remote(ref, ref, hid_near.at[s, j, part], hid_recv.at[s, t, part], (e, sibling))

    def give_back(k):
        s = source(k)
        return remote(
            results.at[s], returned.at[e], ret_send.at[k], ret_recv.at[e], (s, q)
        )

    inputs = [
        pltpu.make_async_copy(there, here, input_sem.at[i])
        for i, (there, here) in enumerate(
            (
                (value_h, value),
                (gate_h, gate),
                (taps_h, taps),
                (ids_h, ids),
                (logits_h, logits),
                (prob_h, prob),
                (gain_h, gain),
                (proj_h, proj),
                (resid_h, resid),
            )
        )
    ]
    loads = []
    for i, (there, here) in enumerate(((w_gate, gate_v), (w_up, up_v))):
        for t in range(n_tp):
            at = (t % 2 * n_y + t // 2) * width
            loads.append(
                pltpu.make_async_copy(
                    there.at[0, pl.ds(t * width, width)],
                    here.at[pl.ds(at, width)],
                    load_sem.at[i * n_tp + t],
                )
            )
    loads.append(pltpu.make_async_copy(w_down.at[0], down_v, load_sem.at[2 * n_tp]))
    for copy in inputs:
        copy.start()
    barrier = pltpu.get_barrier_semaphore()

    @pl.loop(1, n_sp)
    def _(v):
        pl.semaphore_signal(barrier, inc=1, device_id=(moved(v), q), device_id_type=MESH)

    for o in range(1, n_tp):
        pl.semaphore_signal(
            barrier, inc=1, device_id=(e, lax.rem(q + o, n_tp)), device_id_type=MESH
        )
    for copy in inputs[:3]:
        copy.wait()
    for load in loads:
        load.start()

    flow = value[...].astype(jnp.float32) / (1.0 + jnp.exp(-gate[...].astype(jnp.float32)))
    flow = jnp.transpose(flow).astype(jnp.bfloat16)
    halo_out[...] = flow[tokens - history :]
    padded[history:] = flow.astype(jnp.float32)
    lane = lax.broadcasted_iota(jnp.int32, (history, 128), 1)

    def convolve(first):
        filtered = jnp.zeros((history, local), jnp.float32)
        for j in range(taken):
            at = first + history - (taken - 1) + j
            filtered = filtered + taps[j : j + 1] * padded[at : at + history]
        one = jnp.sum(filtered, axis=1, keepdims=True)
        two = jnp.sum(filtered * filtered, axis=1, keepdims=True)
        sums[first : first + history] = jnp.where(lane == 0, one, jnp.where(lane == 1, two, 0.0))
        act[q, first : first + history] = (filtered - one / local).astype(act.dtype)

    sums[0:history] = jnp.zeros((history, 128), jnp.float32)
    for first in range(history, tokens, history):
        convolve(first)
    stats[q] = jnp.transpose(sums[...])[0:8]
    for copy in inputs[3:]:
        copy.wait()
    gains[q] = gain[...]
    pl.semaphore_wait(barrier, n_sp - 1 + n_tp - 1)

    @pl.when(e + 1 < n_sp)
    def _():
        hand_on().start()

    for o in range(1, n_tp):
        tell_gain(o).start()
        tell_stats(o).start()
    for p in range(2):
        for j in range(1, n_y):
            piece(p, q, act_far.at[p, j], far(j)).start()
        piece(p, q, act_near.at[p, 0], sibling).start()

    ahead = lax.broadcasted_iota(jnp.int32, (tokens, tokens), 0)
    after = lax.broadcasted_iota(jnp.int32, (tokens, tokens), 1)
    lanes = max(128, n_sp)
    row_no = lax.broadcasted_iota(jnp.int32, (lanes, tokens), 0)
    row_hit = [jnp.where(row_no == ids[r : r + 1], 1.0, 0.0) for r in range(top)]
    row_rank = jnp.dot(
        sum(row_hit).astype(jnp.bfloat16),
        jnp.where(ahead < after, 1.0, 0.0).astype(jnp.bfloat16),
        preferred_element_type=jnp.float32,
    )
    slot_rows = [
        (ids[r : r + 1] * capacity).astype(jnp.float32)
        + jnp.sum(row_hit[r] * row_rank, axis=0, keepdims=True)
        for r in range(top)
    ]
    for r in range(top):
        slots[r : r + 1] = slot_rows[r]
    slots[top:] = jnp.zeros((slots.shape[0] - top, tokens), jnp.float32)
    share_slots().start()
    scores = logits[...]
    scores = jnp.exp(scores - jnp.max(scores, axis=0, keepdims=True))
    scores = prob[...] * scores / jnp.sum(scores, axis=0, keepdims=True)
    weights[...] = jnp.transpose(sum(row_hit[r] * scores[r : r + 1] for r in range(top)))

    @pl.when(e > 0)
    def _():
        hand_on().wait_recv()
        padded[0:history] = halo_in[...].astype(jnp.float32)

    @pl.when(e == 0)
    def _():
        padded[0:history] = jnp.zeros_like(halo_in).astype(jnp.float32)

    convolve(0)
    stats_head[q] = jnp.transpose(jnp.concatenate([sums[0:history]] * (128 // history), axis=0))[0:8]
    for o in range(1, n_tp):
        tell_head(o).start()
        tell_last(o).start()

    @pl.loop(0, n_sp)
    def _(x):
        place = (x * capacity + lax.broadcasted_iota(jnp.int32, (capacity, tokens), 0)).astype(
            jnp.float32
        )
        chosen = jnp.zeros((capacity, tokens), jnp.float32)
        for r in range(top):
            chosen = chosen + jnp.where(place == slot_rows[r], 1.0, 0.0)
        picks[x] = chosen.astype(picks.dtype)
        picks_back[x] = jnp.transpose(chosen).astype(picks.dtype)

    total[...] = jnp.zeros_like(total)
    channels = proj.shape[0]

    def moments(table, into, turned):
        one = table[0, 0:1]
        two = table[0, 1:2]
        for t in range(1, n_tp):
            one = one + table[t, 0:1]
            two = two + table[t, 1:2]
        mean = one / channels
        scale = lax.rsqrt(two / channels - mean * mean + 1e-05)
        into[...] = jnp.zeros_like(into)
        for t in range(n_tp):
            into[t : t + 1] = (table[t, 0:1] / local - mean) * scale
        into[n_tp : n_tp + 1] = scale
        turned[...] = jnp.transpose(into[...])

    def norm(first, size, turned):
        for t in range(n_tp):
            scaled = act[t, first : first + size].astype(jnp.float32)
            scaled = scaled * turned[first : first + size, n_tp : n_tp + 1]
            scaled = (scaled + turned[first : first + size, t : t + 1]) * gains[t]
            scaled = scaled / (1.0 + jnp.exp(-scaled))
            normal[first : first + size, t * local : (t + 1) * local] = scaled.astype(normal.dtype)

    for o in range(1, n_tp):
        t = lax.rem(q + o, n_tp)
        arrived(stats.at[t], stat_recv.at[t])
        arrived(gains.at[t], gain_recv.at[t])
    moments(stats, flip, columns)
    for p in range(2):
        for j in range(1, n_y):
            t = 2 * below(j) + core
            arrived(piece_at(p, t), act_recv.at[p, t])
            piece(p, t, act_near.at[p, j], sibling).start()
    for p in range(2):
        for j in range(n_y):
            t = 2 * below(j) + (1 - core)
            arrived(piece_at(p, t), act_recv.at[p, t])
        first, size = pieces[p]
        step = 56 if size % 56 == 0 else 16
        for at in range(first, first + size, step):
            norm(at, step, columns)
    for o in range(1, n_tp):
        t = lax.rem(q + o, n_tp)
        arrived(stats_head.at[t], last_recv.at[t])
        arrived(head_at(t), head_recv.at[t])
    moments(stats_head, flip_head, columns_head)
    norm(0, history, columns_head)
    mixed[...] = (
        resid[...].astype(jnp.float32)
        + jnp.dot(normal[...], proj[...], preferred_element_type=jnp.float32)
    ).astype(mixed.dtype)

    def pick(x, block):
        got = jnp.dot(picks[x], block, preferred_element_type=jnp.float32)
        return got.astype(outgoing.dtype)

    if front:
        for j in range(1, n_y):
            share_front(j).start()
    near = 2

    def send(v):
        outgoing[v] = pick(moved(v), mixed[...])
        dispatch(v, e).start()

    def send_front(v):
        for j in range(1, n_y):
            outgoing_front[j - 1, v] = pick(moved(v), mixed_front[above(j)])
            dispatch_front(v, e, j).start()

    def pick_far(d, block):
        got = jnp.dot(picks_far[d], block, preferred_element_type=jnp.float32)
        return got.astype(outgoing.dtype)

    def forward(d):
        outgoing[far_by + d] = pick_far(d, tok[...])
        dispatch(far_by + d, partner).start()

    def forward_front(d):
        for j in range(1, n_y):
            outgoing_front[j - 1, far_by + d] = pick_far(d, tok_front[above(j)])
            dispatch_front(far_by + d, partner, j).start()

    pl.loop(1, near + 1)(send)
    share_tokens().start()
    pl.loop(near + 1, far_by)(send)
    quarter(e, y, 0, width)[...] = pick(e, mixed[...])
    share_slots().wait_recv()

    @pl.loop(0, far_by)
    def _(d):
        place = moved(d) * capacity + lax.broadcasted_iota(jnp.int32, (capacity, tokens), 0)
        chosen = jnp.zeros((capacity, tokens), jnp.float32)
        for r in range(top):
            chosen = chosen + jnp.where(place.astype(jnp.float32) == slots_far[r : r + 1], 1.0, 0.0)
        picks_far[d] = chosen.astype(picks_far.dtype)

    def kinds(k):
        whole = (k < near) | (k == n_sp - 1) if front else k < n_sp
        return ((0, whole), (front, jnp.logical_not(whole)))

    def begin(k):
        s = source(k)
        arrived(quarter(s, y, 0, width), whole_recv.at[s])
        for first, chosen in kinds(k):

            @pl.when(chosen)
            def _():
                for j in range(1, n_y if first < width else 1):
                    cross(s, j, first).start()

    def gather(k):
        s = source(k)
        for first, chosen in kinds(k):

            @pl.when(chosen)
            def _():
                for j in range(1, n_y):
                    of = below(j)
                    if first:

                        @pl.when(order(k) != far_by)
                        def _():
                            arrived(quarter(s, of, 0, first), part_recv.at[s, of])

                    if first < width:
                        arrived(quarter(s, of, first, width - first), cross_recv.at[s, of])

        halve(s).start()

    begin(0)
    for k in range(1, near):
        begin(k)
    for j in range(1, n_y):
        cross(e, j, 0).start()
    if front:
        for j in range(1, n_y):
            arrived(mixed_front.at[below(j)], front_recv.at[below(j)])
        pl.loop(near + 1, far_by)(send_front)
    gather(0)
    for load in loads:
        load.wait()

    tile = min(256, ff_part)
    out_tile = min(256, width)

    def up_step(s):
        @pl.loop(0, parts)
        def _(part):
            @pl.loop(0, ff_part // tile)
            def _(i):
                first = part * ff_part + i * tile
                at = pl.ds(pl.multiple_of(first, tile), tile)
                g = jnp.dot(rows[s], gate_v[:, at], preferred_element_type=jnp.float32)
                u = jnp.dot(rows[s], up_v[:, at], preferred_element_type=jnp.float32)
                h = (g / (1.0 + jnp.exp(-g)) * u).astype(hidden.dtype)
                hidden[s, :, pl.ds(pl.multiple_of(q * ff_local + first, tile), tile)] = h

            for j in range(1, n_y):
                share(s, part, j).start()
            share(s, part, 0).start()

    def down_step(s):
        @pl.loop(0, width // out_tile)
        def _(i):
            at = pl.ds(pl.multiple_of(i * out_tile, out_tile), out_tile)
            o = jnp.dot(hidden[s], down_v[:, at], preferred_element_type=jnp.float32)
            results[s, :, at] = o.astype(results.dtype)

    slot_lane = lax.broadcasted_iota(jnp.int32, weights.shape, 1)

    def combine(x, block):
        got = jnp.dot(picks_back[x], block, preferred_element_type=jnp.float32)
        weight = jnp.sum(jnp.where(slot_lane == x, weights[...], 0.0), axis=1, keepdims=True)
        total[...] += weight * got

    def take(k):
        x = source(k)
        arrived(returned.at[x], ret_recv.at[x])
        combine(x, returned[x])

    def drain(k):
        s = source(k)
        halve(s).wait_send()
        for part in range(parts):
            share(s, part, 0).wait_send()
            for j in range(1, n_y):
                share(s, part, j).wait_send()
                pass_on(s, part, j).wait_send()

        v = order(k)
        for first, chosen in kinds(k):

            @pl.when(chosen)
            def _():
                for j in range(1, n_y if first < width else 1):
                    cross(s, j, first).wait_send()
                if first:

                    @pl.when(v != far_by)
                    def _():
                        for j in range(1, n_y):
                            dispatch_front(v, s, j).wait_send()

        @pl.when((v != far_by) & (v > 0))
        def _():
            dispatch(v, s).wait_send()

    @pl.loop(2, n_sp + 4)
    def _(i):
        @pl.when(i < n_sp + 2)
        def _():
            s = source(i - 2)
            arrived(half(s, 1 - core), half_recv.at[s])
            up_step(s)

        @pl.when(i == 3)
        def _():
            arrived(tok, tok_sem.at[1])
            quarter(partner, y, 0, width)[...] = pick_far(0, tok[...])
            for j in range(1, n_y if front < width else 1):
                cross(partner, j, front).start()
            pl.loop(1, far_by)(forward)

        if front:

            @pl.when(i == 2)
            def _():
                for j in range(1, n_y):
                    share_tokens_front(j).start()

            @pl.when(i == 4)
            def _():
                for j in range(1, n_y):
                    of = below(j)
                    arrived(tok_front.at[of], tok_recv.at[of])
                    quarter(partner, of, 0, front)[...] = pick_far(0, tok_front[of])
                pl.loop(1, far_by)(forward_front)

        @pl.when(i >= 4)
        def _():
            s = source(i - 4)
            for part in range(parts):
                for j in range(n_y):
                    t = 2 * below(j) + (1 - core)
                    arrived(hidden_at(s, t, part), hid_recv.at[s, t, part])
            down_step(s)

            @pl.when(i == n_sp + 3)
            def _():
                combine(e, results[e])

            @pl.when(i < n_sp + 3)
            def _():
                give_back(i - 4).start()

        @pl.when(i < n_sp + 1)
        def _():
            gather(i - 1)

        @pl.when((i >= 3) & (i < n_sp + 3))
        def _():
            s = source(i - 3)
            for part in range(parts):
                for j in range(1, n_y):
                    t = 2 * below(j) + core
                    arrived(hidden_at(s, t, part), hid_recv.at[s, t, part])
                    pass_on(s, part, j).start()

        @pl.when((i >= near) & (i < n_sp - 1) & (order(i) != far_by))
        def _():
            begin(i)

        @pl.when(i >= 5)
        def _():
            drain(i - 5)

        @pl.when(i >= 7)
        def _():
            take(i - 7)

    for k in range(max(0, n_sp - 3), n_sp - 1):
        take(k)
    out[...] = (mixed[...].astype(jnp.float32) + total[...]).astype(out.dtype)

    drain(n_sp - 1)

    @pl.loop(0, n_sp - 1)
    def _(k):
        give_back(k).wait_send()

    @pl.when(e + 1 < n_sp)
    def _():
        hand_on().wait_send()

    for o in range(1, n_tp):
        tell_gain(o).wait_send()
        tell_stats(o).wait_send()
        tell_head(o).wait_send()
        tell_last(o).wait_send()
    for p in range(2):
        piece(p, q, act_near.at[p, 0], sibling).wait_send()
        for j in range(1, n_y):
            piece(p, q, act_far.at[p, j], far(j)).wait_send()
            piece(p, 2 * below(j) + core, act_near.at[p, j], sibling).wait_send()
    share_slots().wait_send()
    share_tokens().wait_send()
    if front:
        for j in range(1, n_y):
            share_front(j).wait_send()
            share_tokens_front(j).wait_send()


def run_layer(value, gate, taps, gain, proj, resid, ids, logits, prob, w_gate, w_up, w_down):
    n_sp, n_tp = lax.axis_size("sp"), lax.axis_size("tp")
    n_y = n_tp // 2
    tokens, width = resid.shape
    local = value.shape[0]
    capacity = 4 * tokens // n_sp
    ff_local = w_gate.shape[2]
    history = -(-(taps.shape[0] - 1) // 16) * 16
    front = width
    span = max(front, 128)
    parts = 2 if ff_local % 512 == 0 else 1
    lanes = max(128, n_sp)
    dma = pltpu.SemaphoreType.DMA
    small = (value, gate, taps, gain, proj, resid, ids, logits, prob)
    return pl.pallas_call(
        functools.partial(expert_kernel, n_sp, n_tp, front),
        out_shape=pltpu.VMEM(resid.shape, resid.dtype),
        in_specs=[pl.BlockSpec(memory_space=pltpu.HBM)] * 12,
        out_specs=pl.BlockSpec(memory_space=pltpu.VMEM),
        scratch_shapes=[pltpu.VMEM(x.shape, x.dtype) for x in small]
        + [
            pltpu.VMEM((history + tokens, local), jnp.float32),
            pltpu.VMEM((tokens, 128), jnp.float32),
            pltpu.VMEM((history, local), jnp.bfloat16),
            pltpu.VMEM((history, local), jnp.bfloat16),
            pltpu.VMEM((n_tp, 1, local), jnp.float32),
            pltpu.VMEM((n_tp, 8, tokens), jnp.float32),
            pltpu.VMEM((n_tp, 8, 128), jnp.float32),
            pltpu.VMEM((128, tokens), jnp.float32),
            pltpu.VMEM((tokens, 128), jnp.float32),
            pltpu.VMEM((128, 128), jnp.float32),
            pltpu.VMEM((128, 128), jnp.float32),
            pltpu.VMEM((n_tp, tokens, local), jnp.bfloat16),
            pltpu.VMEM((tokens, local * n_tp), jnp.bfloat16),
            pltpu.VMEM((tokens, width), jnp.bfloat16),
            pltpu.VMEM((n_y, tokens, span), jnp.bfloat16),
            pltpu.VMEM((8, tokens), jnp.float32),
            pltpu.VMEM((8, tokens), jnp.float32),
            pltpu.VMEM((tokens, width), jnp.bfloat16),
            pltpu.VMEM((n_y, tokens, span), jnp.bfloat16),
            pltpu.VMEM((n_sp, capacity, tokens), jnp.bfloat16),
            pltpu.VMEM((n_sp // 2, capacity, tokens), jnp.bfloat16),
            pltpu.VMEM((n_sp, tokens, capacity), jnp.bfloat16),
            pltpu.VMEM((tokens, lanes), jnp.float32),
            pltpu.VMEM((tokens, width), jnp.float32),
            pltpu.VMEM((n_sp, capacity, width), jnp.bfloat16),
            pltpu.VMEM((n_y - 1 if front else 1, n_sp, capacity, span), jnp.bfloat16),
            pltpu.VMEM((n_sp, capacity, width * n_tp), jnp.bfloat16),
            pltpu.VMEM((n_sp, capacity, ff_local * n_tp), jnp.bfloat16),
            pltpu.VMEM((n_sp, capacity, width), jnp.bfloat16),
            pltpu.VMEM((n_sp, capacity, width), jnp.bfloat16),
            pltpu.VMEM(w_gate.shape[1:], jnp.bfloat16),
            pltpu.VMEM(w_up.shape[1:], jnp.bfloat16),
            pltpu.VMEM(w_down.shape[1:], jnp.bfloat16),
            dma((len(small),)),
            dma((2 * n_tp + 1,)),
            dma((2,)),
        ]
        + [dma((n_tp,))] * 8
        + [
            dma((2, n_tp)),
            dma((2, n_y)),
            dma((2, n_y)),
            dma((n_y,)),
            dma((n_y,)),
            dma((2,)),
            dma((2,)),
            dma((n_y,)),
            dma((n_y,)),
            dma((n_sp,)),
            dma((n_sp,)),
            dma((n_sp, n_y)),
            dma((n_sp, n_y)),
            dma((n_sp, n_y)),
            dma((n_sp, n_y)),
            dma((n_sp,)),
            dma((n_sp,)),
            dma((n_sp, n_tp, parts)),
            dma((n_sp, n_y, parts)),
            dma((n_sp, n_y, parts)),
            dma((n_sp,)),
            dma((n_sp,)),
        ],
        compiler_params=pltpu.CompilerParams(
            collective_id=0, has_side_effects=True, vmem_limit_bytes=57000000
        ),
    )(*small, w_gate, w_up, w_down)


def per_device(
    glu_value,
    glu_gate,
    conv_taps,
    norm_gain,
    out_proj,
    resid,
    expert_ids,
    route_logits,
    group_prob,
    w_gate,
    w_up,
    w_down,
):
    return run_layer(
        glu_value,
        glu_gate,
        conv_taps.T,
        norm_gain[None, :],
        out_proj,
        resid,
        expert_ids.T,
        route_logits.T,
        group_prob[None, :],
        w_gate,
        w_up,
        w_down,
    )


def solution(mesh):
    return jax.shard_map(
        per_device,
        mesh=mesh,
        in_specs=(
            P("tp", "sp"),
            P("tp", "sp"),
            P("tp", None),
            P("tp"),
            P(None, "tp"),
            P("sp", "tp"),
            P("sp", None),
            P("sp", None),
            P("sp"),
            P("sp", None, "tp"),
            P("sp", None, "tp"),
            P("sp", None, "tp"),
        ),
        out_specs=P("sp", "tp"),
        check_vma=False,
    )
```

```python
import functools

import jax
import jax.numpy as jnp
from jax import lax
from jax.experimental import pallas as pl
from jax.experimental.pallas import tpu as pltpu
from jax.sharding import PartitionSpec as P

MESH = pl.DeviceIdType.MESH


def expert_kernel(
    n_sp,
    n_tp,
    value_h,
    gate_h,
    taps_h,
    gain_h,
    proj_h,
    resid_h,
    ids_h,
    logits_h,
    prob_h,
    w_gate,
    w_up,
    w_down,
    out,
    value,
    gate,
    taps,
    gain,
    proj,
    resid,
    ids,
    logits,
    prob,
    padded,
    sums,
    halo_out,
    halo_in,
    stats,
    stats_head,
    flip,
    columns,
    flip_head,
    columns_head,
    act,
    normal,
    mixed,
    mixed_front,
    slots,
    slots_far,
    tok,
    tok_front,
    picks,
    picks_far,
    picks_back,
    weights,
    total,
    outgoing,
    outgoing_front,
    rows,
    hidden,
    results,
    returned,
    gate_v,
    up_v,
    down_v,
    input_sem,
    load_sem,
    halo_sem,
    stat_send,
    stat_recv,
    head_send,
    head_recv,
    last_send,
    last_recv,
    act_recv,
    act_side,
    act_send,
    front_send,
    front_recv,
    slot_sem,
    tok_sem,
    tok_send,
    tok_recv,
    whole_send,
    whole_recv,
    cross_send,
    cross_recv,
    half_send,
    half_recv,
    hid_recv,
    hid_side,
    hid_send,
    ret_send,
    ret_recv,
):
    e = lax.axis_index("sp")
    q = lax.axis_index("tp")
    n_y = n_tp // 2
    y, core = q // 2, q % 2
    sibling = 2 * y + (1 - core)
    _, capacity, width = results.shape
    tokens = mixed.shape[0]
    ff_local = gate_v.shape[1]
    parts = hid_recv.shape[2]
    near = cross_send.shape[0]
    ff_part = ff_local // parts
    history, local = halo_in.shape
    taken = taps.shape[0]
    top = ids.shape[0]
    middle = history + (tokens - history) // 32 * 16
    pieces = ((history, middle - history), (middle, tokens - middle))
    far_by = n_sp // 2
    bits = [e // 2**b % 2 for b in range(n_sp.bit_length() - 1)]

    def moved(v):
        return sum((bits[b] + v // 2**b) % 2 * 2**b for b in range(len(bits)))

    def order(k):
        return lax.rem(k + 1, n_sp)

    def source(k):
        return moved(order(k))

    partner = moved(far_by)

    def far(j):
        return 2 * lax.rem(y + j, n_y) + core

    def above(j):
        return lax.rem(y + j, n_y)

    def below(j):
        return lax.rem(y + n_y - j, n_y)

    def quarter(s, of, first, size):
        at = pl.multiple_of((core * n_y + of) * width + first, min(128, width))
        return rows.at[s, :, pl.ds(at, size)]

    def half(s, c):
        return rows.at[s, :, pl.ds(pl.multiple_of(c * n_y * width, width), n_y * width)]

    def hidden_at(s, t, part):
        at = pl.multiple_of(t * ff_local + part * ff_part, ff_part)
        return hidden.at[s, :, pl.ds(at, ff_part)]

    def remote(src, dst, send, recv, to):
        return pltpu.make_async_remote_copy(
            src_ref=src,
            dst_ref=dst,
            send_sem=send,
            recv_sem=recv,
            device_id=to,
            device_id_type=MESH,
        )

    def arrived(ref, recv):
        pltpu.make_async_copy(ref, ref, recv).wait()

    def tell(o, ref, send, recv):
        return remote(ref, ref, send.at[0], recv.at[0], (e, lax.rem(q + o, n_tp)))

    def tell_stats(o):
        return tell(o, stats.at[q], stat_send, stat_recv)

    def tell_last(o):
        return tell(o, stats_head.at[q], last_send, last_recv)

    def tell_head(o):
        return tell(o, act.at[q, pl.ds(0, history)], head_send, head_recv)

    others = pl.ds(0, n_tp - 1)
    sent = pl.ds(0, 2 * n_y - 1)
    all_stats = stats.at[others]
    all_last = stats_head.at[others]
    all_heads = act.at[others, pl.ds(0, history)]
    all_pieces = act.at[sent, pl.ds(history, tokens - history)]

    def hand_on():
        to = (lax.rem(e + 1, n_sp), q)
        return remote(halo_out, halo_in, halo_sem.at[0], halo_sem.at[1], to)

    def piece_at(p, t):
        return act.at[t, pl.ds(pieces[p][0], pieces[p][1])]

    def piece(p, j):
        ref = piece_at(p, q)
        if j == 0:
            return remote(ref, ref, act_send.at[0], act_side.at[p], (e, sibling))
        return remote(ref, ref, act_send.at[0], act_recv.at[p, j - 1], (e, far(j)))

    def pass_piece(p, j):
        ref = piece_at(p, 2 * below(j) + core)
        return remote(ref, ref, act_send.at[0], act_side.at[p], (e, sibling))

    def share_front(j):
        return remote(mixed, mixed_front.at[y], front_send.at[0], front_recv.at[0], (e, far(j)))

    all_fronts = mixed_front.at[pl.ds(0, n_y - 1)]

    def share_slots():
        return remote(slots, slots_far, slot_sem.at[0], slot_sem.at[1], (partner, q))

    def share_tokens():
        return remote(mixed, tok, tok_sem.at[0], tok_sem.at[1], (partner, q))

    def share_tokens_front(j):
        of = above(j)
        ours = mixed_front.at[of]
        return remote(ours, tok_front.at[of], tok_send.at[0], tok_recv.at[0], (partner, q))

    all_tokens = tok_front.at[pl.ds(0, n_y - 1)]

    def dispatch(v, s, kind):
        to = moved(lax.rem(v, far_by))
        return remote(
            outgoing.at[v],
            quarter(s, y, 0, width),
            whole_send.at[kind],
            whole_recv.at[s],
            (to, q),
        )

    def dispatch_front(v, s, j):
        to = moved(lax.rem(v, far_by))
        of = above(j)
        return remote(
            outgoing_front.at[j - 1, v],
            quarter(s, of, 0, width),
            whole_send.at[1],
            whole_recv.at[s],
            (to, q),
        )

    def cross(k, j):
        ref = quarter(source(k), y, 0, width)
        return remote(ref, ref, cross_send.at[k, j - 1], cross_recv.at[k, j - 1], (e, far(j)))

    def halve(s):
        ref = half(s, core)
        return remote(ref, ref, half_send.at[0], half_recv.at[s], (e, sibling))

    def share(s, part, j):
        ref = hidden_at(s, q, part)
        if j == 0:
            return remote(ref, ref, hid_send.at[0], hid_side.at[s], (e, sibling))
        return remote(ref, ref, hid_send.at[0], hid_recv.at[s, j - 1, part], (e, far(j)))

    def pass_on(s, part, j):
        ref = hidden_at(s, 2 * below(j) + core, part)
        return remote(ref, ref, hid_send.at[0], hid_side.at[s], (e, sibling))

    def hidden_bytes(s, blocks):
        return hidden.at[s, :, pl.ds(0, blocks * ff_local)]

    def give_back(k):
        s = source(k)
        return remote(
            results.at[s], returned.at[e], ret_send.at[0], ret_recv.at[e], (s, q)
        )

    inputs = [
        pltpu.make_async_copy(there, here, input_sem.at[i])
        for i, (there, here) in enumerate(
            (
                (value_h, value),
                (gate_h, gate),
                (taps_h, taps),
                (ids_h, ids),
                (logits_h, logits),
                (prob_h, prob),
                (gain_h, gain),
                (proj_h, proj),
                (resid_h, resid),
            )
        )
    ]
    loads = []
    for i, (there, here) in enumerate(((w_gate, gate_v), (w_up, up_v))):
        for t in range(n_tp):
            at = (t % 2 * n_y + t // 2) * width
            loads.append(
                pltpu.make_async_copy(
                    there.at[0, pl.ds(t * width, width)],
                    here.at[pl.ds(at, width)],
                    load_sem.at[i],
                )
            )
    loads.append(pltpu.make_async_copy(w_down.at[0], down_v, load_sem.at[2]))
    for copy in inputs:
        copy.start()
    barrier = pltpu.get_barrier_semaphore()

    @pl.loop(1, n_sp)
    def _(v):
        pl.semaphore_signal(barrier, inc=1, device_id=(moved(v), q), device_id_type=MESH)

    for o in range(1, n_tp):
        pl.semaphore_signal(
            barrier, inc=1, device_id=(e, lax.rem(q + o, n_tp)), device_id_type=MESH
        )
    for copy in inputs[:3]:
        copy.wait()
    for load in loads:
        load.start()

    flow = value[...].astype(jnp.float32) / (1.0 + jnp.exp(-gate[...].astype(jnp.float32)))
    flow = jnp.transpose(flow).astype(jnp.bfloat16)
    halo_out[...] = flow[tokens - history :]
    padded[history:] = flow.astype(jnp.float32)
    lane = lax.broadcasted_iota(jnp.int32, (history, 128), 1)

    def convolve(first):
        filtered = jnp.zeros((history, local), jnp.float32)
        for j in range(taken):
            at = first + history - (taken - 1) + j
            filtered = filtered + taps[j : j + 1] * padded[at : at + history]
        one = jnp.sum(filtered, axis=1, keepdims=True)
        two = jnp.sum(filtered * filtered, axis=1, keepdims=True)
        sums[first : first + history] = jnp.where(lane == 0, one, jnp.where(lane == 1, two, 0.0))
        act[q, first : first + history] = (filtered - one / local).astype(act.dtype)

    sums[0:history] = jnp.zeros((history, 128), jnp.float32)
    for first in range(history, middle, history):
        convolve(first)
    pl.semaphore_wait(barrier, n_sp - 1 + n_tp - 1)

    @pl.when(e + 1 < n_sp)
    def _():
        hand_on().start()

    for j in range(n_y - 1, -1, -1):
        piece(0, j).start()
    for first in range(first + history, tokens, history):
        convolve(first)
    for copy in inputs[3:]:
        copy.wait()
    stats[q, 0:8] = jnp.transpose(sums[...])[0:8]
    stats[q, 8:9, 0:local] = gain[...]
    for o in range(1, n_tp):
        tell_stats(o).start()
    for j in range(n_y - 1, -1, -1):
        piece(1, j).start()

    ahead = lax.broadcasted_iota(jnp.int32, (tokens, tokens), 0)
    after = lax.broadcasted_iota(jnp.int32, (tokens, tokens), 1)
    lanes = max(128, n_sp)
    row_no = lax.broadcasted_iota(jnp.int32, (lanes, tokens), 0)
    row_hit = [jnp.where(row_no == ids[r : r + 1], 1.0, 0.0) for r in range(top)]
    row_rank = jnp.dot(
        sum(row_hit).astype(jnp.bfloat16),
        jnp.where(ahead < after, 1.0, 0.0).astype(jnp.bfloat16),
        preferred_element_type=jnp.float32,
    )
    slot_rows = [
        (ids[r : r + 1] * capacity).astype(jnp.float32)
        + jnp.sum(row_hit[r] * row_rank, axis=0, keepdims=True)
        for r in range(top)
    ]
    for r in range(top):
        slots[r : r + 1] = slot_rows[r]
    slots[top:] = jnp.zeros((slots.shape[0] - top, tokens), jnp.float32)
    share_slots().start()
    scores = logits[...]
    scores = jnp.exp(scores - jnp.max(scores, axis=0, keepdims=True))
    scores = prob[...] * scores / jnp.sum(scores, axis=0, keepdims=True)
    weights[...] = jnp.transpose(sum(row_hit[r] * scores[r : r + 1] for r in range(top)))

    @pl.when(e > 0)
    def _():
        hand_on().wait_recv()
        padded[0:history] = halo_in[...].astype(jnp.float32)

    @pl.when(e == 0)
    def _():
        padded[0:history] = jnp.zeros_like(halo_in).astype(jnp.float32)

    convolve(0)
    stats_head[q] = jnp.transpose(jnp.concatenate([sums[0:history]] * (128 // history), axis=0))[0:8]
    for o in range(1, n_tp):
        tell_head(o).start()
        tell_last(o).start()

    @pl.loop(0, n_sp)
    def _(x):
        place = (x * capacity + lax.broadcasted_iota(jnp.int32, (capacity, tokens), 0)).astype(
            jnp.float32
        )
        chosen = jnp.zeros((capacity, tokens), jnp.float32)
        for r in range(top):
            chosen = chosen + jnp.where(place == slot_rows[r], 1.0, 0.0)
        picks[x] = chosen.astype(picks.dtype)
        picks_back[x] = jnp.transpose(chosen).astype(picks.dtype)

    total[...] = jnp.zeros_like(total)
    channels = proj.shape[0]

    def moments(table, into, turned):
        one = table[0, 0:1]
        two = table[0, 1:2]
        for t in range(1, n_tp):
            one = one + table[t, 0:1]
            two = two + table[t, 1:2]
        mean = one / channels
        scale = lax.rsqrt(two / channels - mean * mean + 1e-05)
        into[...] = jnp.zeros_like(into)
        for t in range(n_tp):
            into[t : t + 1] = (table[t, 0:1] / local - mean) * scale
        into[n_tp : n_tp + 1] = scale
        turned[...] = jnp.transpose(into[...])

    def norm(first, size, turned):
        for t in range(n_tp):
            scaled = act[t, first : first + size].astype(jnp.float32)
            scaled = scaled * turned[first : first + size, n_tp : n_tp + 1]
            scaled = (scaled + turned[first : first + size, t : t + 1]) * stats[t, 8:9, 0:local]
            scaled = scaled / (1.0 + jnp.exp(-scaled))
            normal[first : first + size, t * local : (t + 1) * local] = scaled.astype(normal.dtype)

    arrived(all_stats, stat_recv.at[0])
    moments(stats, flip, columns)
    for p in range(2):
        for j in range(1, n_y):
            arrived(piece_at(p, 2 * below(j) + core), act_recv.at[p, j - 1])
            pass_piece(p, j).start()
    for p in range(2):
        first, size = pieces[p]
        arrived(act.at[pl.ds(0, n_y), pl.ds(first, size)], act_side.at[p])
        step = 56 if size % 56 == 0 else 16
        for at in range(first, first + size, step):
            norm(at, step, columns)
    arrived(all_last, last_recv.at[0])
    arrived(all_heads, head_recv.at[0])
    moments(stats_head, flip_head, columns_head)
    norm(0, history, columns_head)
    mixed[...] = (
        resid[...].astype(jnp.float32)
        + jnp.dot(normal[...], proj[...], preferred_element_type=jnp.float32)
    ).astype(mixed.dtype)

    def pick(x, block):
        got = jnp.dot(picks[x], block, preferred_element_type=jnp.float32)
        return got.astype(outgoing.dtype)

    for j in range(1, n_y):
        share_front(j).start()

    def send(v, kind):
        outgoing[v] = pick(moved(v), mixed[...])
        dispatch(v, e, kind).start()

    def send_front(v):
        for j in range(1, n_y):
            outgoing_front[j - 1, v] = pick(moved(v), mixed_front[above(j)])
            dispatch_front(v, e, j).start()

    def pick_far(d, block):
        got = jnp.dot(picks_far[d], block, preferred_element_type=jnp.float32)
        return got.astype(outgoing.dtype)

    def forward(d):
        outgoing[far_by + d] = pick_far(d, tok[...])
        dispatch(far_by + d, partner, 1).start()

    def forward_front(d):
        for j in range(1, n_y):
            outgoing_front[j - 1, far_by + d] = pick_far(d, tok_front[above(j)])
            dispatch_front(far_by + d, partner, j).start()

    pl.loop(1, near + 1)(functools.partial(send, kind=0))
    share_tokens().start()
    pl.loop(near + 1, far_by)(functools.partial(send, kind=1))
    quarter(e, y, 0, width)[...] = pick(e, mixed[...])
    share_slots().wait_recv()

    @pl.loop(0, far_by)
    def _(d):
        place = moved(d) * capacity + lax.broadcasted_iota(jnp.int32, (capacity, tokens), 0)
        chosen = jnp.zeros((capacity, tokens), jnp.float32)
        for r in range(top):
            chosen = chosen + jnp.where(place.astype(jnp.float32) == slots_far[r : r + 1], 1.0, 0.0)
        picks_far[d] = chosen.astype(picks_far.dtype)

    def begin(k):
        s = source(k)
        arrived(quarter(s, y, 0, width), whole_recv.at[s])
        for j in range(1, n_y):
            cross(k, j).start()

    def gather(k):
        s = source(k)

        @pl.when(k < near)
        def _():
            for j in range(1, n_y):
                arrived(quarter(s, below(j), 0, width), cross_recv.at[k, j - 1])

        @pl.when((k >= near) & (s != e) & (s != partner))
        def _():
            arrived(half(s, core), whole_recv.at[s])

        halve(s).start()

    for k in range(near):
        begin(k)
    arrived(all_fronts, front_recv.at[0])
    pl.loop(near + 1, far_by)(send_front)
    for j in range(1, n_y):
        of = below(j)
        quarter(e, of, 0, width)[...] = pick(e, mixed_front[of])
    gather(0)
    for j in range(1, n_y):
        share_tokens_front(j).start()
    arrived(gate_v, load_sem.at[0])
    arrived(up_v, load_sem.at[1])
    loads[-1].wait()

    tile = min(256, ff_part)
    out_tile = min(256, width)

    def up_step(s):
        @pl.loop(0, parts)
        def _(part):
            @pl.loop(0, ff_part // tile)
            def _(i):
                first = part * ff_part + i * tile
                at = pl.ds(pl.multiple_of(first, tile), tile)
                g = jnp.dot(rows[s], gate_v[:, at], preferred_element_type=jnp.float32)
                u = jnp.dot(rows[s], up_v[:, at], preferred_element_type=jnp.float32)
                h = (g / (1.0 + jnp.exp(-g)) * u).astype(hidden.dtype)
                hidden[s, :, pl.ds(pl.multiple_of(q * ff_local + first, tile), tile)] = h

            for j in range(1, n_y):
                share(s, part, j).start()
            share(s, part, 0).start()

    def down_step(s):
        @pl.loop(0, width // out_tile)
        def _(i):
            at = pl.ds(pl.multiple_of(i * out_tile, out_tile), out_tile)
            o = jnp.dot(hidden[s], down_v[:, at], preferred_element_type=jnp.float32)
            results[s, :, at] = o.astype(results.dtype)

    slot_lane = lax.broadcasted_iota(jnp.int32, weights.shape, 1)

    def combine(x, block):
        got = jnp.dot(picks_back[x], block, preferred_element_type=jnp.float32)
        weight = jnp.sum(jnp.where(slot_lane == x, weights[...], 0.0), axis=1, keepdims=True)
        total[...] += weight * got

    def take(k):
        x = source(k)
        arrived(returned.at[x], ret_recv.at[x])
        combine(x, returned[x])

    @pl.loop(2, n_sp + 4)
    def _(i):
        @pl.when(i == n_sp + 3)
        def _():
            take(n_sp - 3)

        @pl.when(i < n_sp + 2)
        def _():
            s = source(i - 2)
            arrived(half(s, 1 - core), half_recv.at[s])
            up_step(s)

        @pl.when(i == 3)
        def _():
            arrived(tok, tok_sem.at[1])
            quarter(partner, y, 0, width)[...] = pick_far(0, tok[...])
            pl.loop(1, far_by)(forward)

        @pl.when(i == 4)
        def _():
            arrived(all_tokens, tok_recv.at[0])
            for j in range(1, n_y):
                of = below(j)
                quarter(partner, of, 0, width)[...] = pick_far(0, tok_front[of])
            pl.loop(1, far_by)(forward_front)

        @pl.when(i >= 4)
        def _():
            s = source(i - 4)
            arrived(hidden_bytes(s, n_y), hid_side.at[s])
            down_step(s)

            @pl.when(i == n_sp + 3)
            def _():
                combine(e, results[e])

            @pl.when(i < n_sp + 3)
            def _():
                give_back(i - 4).start()

        @pl.when(i < n_sp + 1)
        def _():
            gather(i - 1)

        @pl.when((i >= 3) & (i < n_sp + 3))
        def _():
            s = source(i - 3)
            for part in range(parts):
                for j in range(1, n_y):
                    t = 2 * below(j) + core
                    arrived(hidden_at(s, t, part), hid_recv.at[s, j - 1, part])
                    pass_on(s, part, j).start()

        @pl.when((i >= 6) & (i < n_sp + 3))
        def _():
            take(i - 6)

    for k in range(max(0, n_sp - 2), n_sp - 1):
        take(k)
    out[...] = (mixed[...].astype(jnp.float32) + total[...]).astype(out.dtype)

    every = pl.ds(0, n_sp)
    for k in range(near):
        for j in range(1, n_y):
            cross(k, j).wait_send()
    arrived(outgoing.at[pl.ds(0, near)], whole_send.at[0])
    rest = pl.ds(0, n_sp - 2 - near)
    arrived(rows.at[rest, :, pl.ds(0, n_y * width)], whole_send.at[1])
    arrived(rows.at[every, :, pl.ds(0, n_y * width)], half_send.at[0])
    arrived(hidden.at[every, :, pl.ds(0, (2 * n_y - 1) * ff_local)], hid_send.at[0])
    arrived(results.at[pl.ds(0, n_sp - 1)], ret_send.at[0])

    @pl.when(e + 1 < n_sp)
    def _():
        hand_on().wait_send()

    arrived(all_stats, stat_send.at[0])
    arrived(all_last, last_send.at[0])
    arrived(all_heads, head_send.at[0])
    arrived(all_pieces, act_send.at[0])
    share_slots().wait_send()
    share_tokens().wait_send()
    arrived(all_fronts, front_send.at[0])
    arrived(all_tokens, tok_send.at[0])


def run_layer(value, gate, taps, gain, proj, resid, ids, logits, prob, w_gate, w_up, w_down):
    n_sp, n_tp = lax.axis_size("sp"), lax.axis_size("tp")
    n_y = n_tp // 2
    tokens, width = resid.shape
    local = value.shape[0]
    capacity = 4 * tokens // n_sp
    ff_local = w_gate.shape[2]
    history = -(-(taps.shape[0] - 1) // 16) * 16
    parts = 2 if ff_local % 512 == 0 else 1
    lanes = max(128, n_sp)
    dma = pltpu.SemaphoreType.DMA
    small = (value, gate, taps, gain, proj, resid, ids, logits, prob)
    return pl.pallas_call(
        functools.partial(expert_kernel, n_sp, n_tp),
        out_shape=pltpu.VMEM(resid.shape, resid.dtype),
        in_specs=[pl.BlockSpec(memory_space=pltpu.HBM)] * 12,
        out_specs=pl.BlockSpec(memory_space=pltpu.VMEM),
        scratch_shapes=[pltpu.VMEM(x.shape, x.dtype) for x in small]
        + [
            pltpu.VMEM((history + tokens, local), jnp.float32),
            pltpu.VMEM((tokens, 128), jnp.float32),
            pltpu.VMEM((history, local), jnp.bfloat16),
            pltpu.VMEM((history, local), jnp.bfloat16),
            pltpu.VMEM((n_tp, 16, tokens), jnp.float32),
            pltpu.VMEM((n_tp, 8, 128), jnp.float32),
            pltpu.VMEM((128, tokens), jnp.float32),
            pltpu.VMEM((tokens, 128), jnp.float32),
            pltpu.VMEM((128, 128), jnp.float32),
            pltpu.VMEM((128, 128), jnp.float32),
            pltpu.VMEM((n_tp, tokens, local), jnp.bfloat16),
            pltpu.VMEM((tokens, local * n_tp), jnp.bfloat16),
            pltpu.VMEM((tokens, width), jnp.bfloat16),
            pltpu.VMEM((n_y, tokens, width), jnp.bfloat16),
            pltpu.VMEM((8, tokens), jnp.float32),
            pltpu.VMEM((8, tokens), jnp.float32),
            pltpu.VMEM((tokens, width), jnp.bfloat16),
            pltpu.VMEM((n_y, tokens, width), jnp.bfloat16),
            pltpu.VMEM((n_sp, capacity, tokens), jnp.bfloat16),
            pltpu.VMEM((n_sp // 2, capacity, tokens), jnp.bfloat16),
            pltpu.VMEM((n_sp, tokens, capacity), jnp.bfloat16),
            pltpu.VMEM((tokens, lanes), jnp.float32),
            pltpu.VMEM((tokens, width), jnp.float32),
            pltpu.VMEM((n_sp, capacity, width), jnp.bfloat16),
            pltpu.VMEM((n_y - 1, n_sp, capacity, width), jnp.bfloat16),
            pltpu.VMEM((n_sp, capacity, width * n_tp), jnp.bfloat16),
            pltpu.VMEM((n_sp, capacity, ff_local * n_tp), jnp.bfloat16),
            pltpu.VMEM((n_sp, capacity, width), jnp.bfloat16),
            pltpu.VMEM((n_sp, capacity, width), jnp.bfloat16),
            pltpu.VMEM(w_gate.shape[1:], jnp.bfloat16),
            pltpu.VMEM(w_up.shape[1:], jnp.bfloat16),
            pltpu.VMEM(w_down.shape[1:], jnp.bfloat16),
            dma((len(small),)),
            dma((3,)),
            dma((2,)),
        ]
        + [dma((1,))] * 6
        + [
            dma((2, n_y - 1)),
            dma((2,)),
            dma((1,)),
            dma((1,)),
            dma((1,)),
            dma((2,)),
            dma((2,)),
            dma((1,)),
            dma((1,)),
            dma((2,)),
            dma((n_sp,)),
            dma((2, n_y - 1)),
            dma((2, n_y - 1)),
            dma((1,)),
            dma((n_sp,)),
            dma((n_sp, n_y - 1, parts)),
            dma((n_sp,)),
            dma((1,)),
            dma((1,)),
            dma((n_sp,)),
        ],
        compiler_params=pltpu.CompilerParams(
            collective_id=0, has_side_effects=True, vmem_limit_bytes=57000000
        ),
    )(*small, w_gate, w_up, w_down)


def per_device(
    glu_value,
    glu_gate,
    conv_taps,
    norm_gain,
    out_proj,
    resid,
    expert_ids,
    route_logits,
    group_prob,
    w_gate,
    w_up,
    w_down,
):
    return run_layer(
        glu_value,
        glu_gate,
        conv_taps.T,
        norm_gain[None, :],
        out_proj,
        resid,
        expert_ids.T,
        route_logits.T,
        group_prob[None, :],
        w_gate,
        w_up,
        w_down,
    )


def solution(mesh):
    return jax.shard_map(
        per_device,
        mesh=mesh,
        in_specs=(
            P("tp", "sp"),
            P("tp", "sp"),
            P("tp", None),
            P("tp"),
            P(None, "tp"),
            P("sp", "tp"),
            P("sp", None),
            P("sp", None),
            P("sp"),
            P("sp", None, "tp"),
            P("sp", None, "tp"),
            P("sp", None, "tp"),
        ),
        out_specs=P("sp", "tp"),
        check_vma=False,
    )
```

```python
import functools

import jax
import jax.numpy as jnp
from jax import lax
from jax.experimental import pallas as pl
from jax.experimental.pallas import tpu as pltpu
from jax.sharding import PartitionSpec as P

MESH = pl.DeviceIdType.MESH


def expert_kernel(
    n_sp,
    n_tp,
    value_h,
    gate_h,
    taps_h,
    gain_h,
    proj_h,
    resid_h,
    ids_h,
    logits_h,
    prob_h,
    w_gate,
    w_up,
    w_down,
    out,
    value,
    gate,
    taps,
    gain,
    proj,
    resid,
    ids,
    logits,
    prob,
    padded,
    sums,
    halo_out,
    halo_in,
    stats,
    stats_head,
    flip,
    columns,
    flip_head,
    columns_head,
    act,
    normal,
    mixed,
    mixed_front,
    slots,
    slots_far,
    tok,
    tok_front,
    picks,
    picks_far,
    picks_back,
    weights,
    total,
    outgoing,
    outgoing_front,
    rows,
    hidden,
    results,
    returned,
    gate_v,
    up_v,
    down_v,
    input_sem,
    load_sem,
    halo_sem,
    stat_send,
    stat_recv,
    head_send,
    head_recv,
    last_send,
    last_recv,
    act_recv,
    act_side,
    act_send,
    front_send,
    front_recv,
    slot_sem,
    tok_sem,
    tok_send,
    tok_recv,
    whole_send,
    whole_recv,
    cross_send,
    cross_recv,
    half_send,
    half_recv,
    hid_recv,
    hid_side,
    hid_send,
    ret_send,
    ret_recv,
):
    e = lax.axis_index("sp")
    q = lax.axis_index("tp")
    n_y = n_tp // 2
    y, core = q // 2, q % 2
    sibling = 2 * y + (1 - core)
    _, capacity, width = results.shape
    tokens = mixed.shape[0]
    ff_local = gate_v.shape[1]
    parts = hid_recv.shape[2]
    near = cross_send.shape[0]
    ff_part = ff_local // parts
    history, local = halo_in.shape
    taken = taps.shape[0]
    top = ids.shape[0]
    middle = history + (tokens - history) // 32 * 16
    pieces = ((history, middle - history), (middle, tokens - middle))
    far_by = n_sp // 2
    bits = [e // 2**b % 2 for b in range(n_sp.bit_length() - 1)]

    def moved(v):
        return sum((bits[b] + v // 2**b) % 2 * 2**b for b in range(len(bits)))

    def order(k):
        return lax.rem(k + 1, n_sp)

    def source(k):
        return moved(order(k))

    partner = moved(far_by)

    def far(j):
        return 2 * lax.rem(y + j, n_y) + core

    def above(j):
        return lax.rem(y + j, n_y)

    def below(j):
        return lax.rem(y + n_y - j, n_y)

    def quarter(s, of, first, size):
        at = pl.multiple_of((core * n_y + of) * width + first, min(128, width))
        return rows.at[s, :, pl.ds(at, size)]

    def half(s, c):
        return rows.at[s, :, pl.ds(pl.multiple_of(c * n_y * width, width), n_y * width)]

    def hidden_at(s, t, part):
        at = pl.multiple_of(t * ff_local + part * ff_part, ff_part)
        return hidden.at[s, :, pl.ds(at, ff_part)]

    def remote(src, dst, send, recv, to):
        return pltpu.make_async_remote_copy(
            src_ref=src,
            dst_ref=dst,
            send_sem=send,
            recv_sem=recv,
            device_id=to,
            device_id_type=MESH,
        )

    def arrived(ref, recv):
        pltpu.make_async_copy(ref, ref, recv).wait()

    def tell(o, ref, send, recv):
        return remote(ref, ref, send.at[0], recv.at[0], (e, lax.rem(q + o, n_tp)))

    def tell_stats(o):
        return tell(o, stats.at[q], stat_send, stat_recv)

    def tell_last(o):
        return tell(o, stats_head.at[q], last_send, last_recv)

    def tell_head(o):
        return tell(o, act.at[q, pl.ds(0, history)], head_send, head_recv)

    others = pl.ds(0, n_tp - 1)
    sent = pl.ds(0, 2 * n_y - 1)
    all_stats = stats.at[others]
    all_last = stats_head.at[others]
    all_heads = act.at[others, pl.ds(0, history)]
    all_pieces = act.at[sent, pl.ds(history, tokens - history)]

    def hand_on():
        to = (lax.rem(e + 1, n_sp), q)
        return remote(halo_out, halo_in, halo_sem.at[0], halo_sem.at[1], to)

    def piece_at(p, t):
        return act.at[t, pl.ds(pieces[p][0], pieces[p][1])]

    def piece(p, j):
        ref = piece_at(p, q)
        if j == 0:
            return remote(ref, ref, act_send.at[0], act_side.at[p], (e, sibling))
        return remote(ref, ref, act_send.at[0], act_recv.at[p, j - 1], (e, far(j)))

    def pass_piece(p, j):
        ref = piece_at(p, 2 * below(j) + core)
        return remote(ref, ref, act_send.at[0], act_side.at[p], (e, sibling))

    def share_front(j):
        return remote(mixed, mixed_front.at[y], front_send.at[0], front_recv.at[0], (e, far(j)))

    all_fronts = mixed_front.at[pl.ds(0, n_y - 1)]

    def share_slots():
        return remote(slots, slots_far, slot_sem.at[0], slot_sem.at[1], (partner, q))

    def share_tokens():
        return remote(mixed, tok, tok_sem.at[0], tok_sem.at[1], (partner, q))

    def share_tokens_front(j):
        of = above(j)
        ours = mixed_front.at[of]
        return remote(ours, tok_front.at[of], tok_send.at[0], tok_recv.at[0], (partner, q))

    all_tokens = tok_front.at[pl.ds(0, n_y - 1)]

    def dispatch(v, s, kind):
        to = moved(lax.rem(v, far_by))
        return remote(
            outgoing.at[v],
            quarter(s, y, 0, width),
            whole_send.at[kind],
            whole_recv.at[s],
            (to, q),
        )

    def dispatch_front(v, s, j):
        to = moved(lax.rem(v, far_by))
        of = above(j)
        return remote(
            outgoing_front.at[j - 1, v],
            quarter(s, of, 0, width),
            whole_send.at[1],
            whole_recv.at[s],
            (to, q),
        )

    def cross(k, j):
        ref = quarter(source(k), y, 0, width)
        return remote(ref, ref, cross_send.at[k, j - 1], cross_recv.at[k, j - 1], (e, far(j)))

    def halve(s):
        ref = half(s, core)
        return remote(ref, ref, half_send.at[0], half_recv.at[s], (e, sibling))

    def share(s, part, j):
        ref = hidden_at(s, q, part)
        if j == 0:
            return remote(ref, ref, hid_send.at[0], hid_side.at[s], (e, sibling))
        return remote(ref, ref, hid_send.at[0], hid_recv.at[s, j - 1, part], (e, far(j)))

    def pass_on(s, part, j):
        ref = hidden_at(s, 2 * below(j) + core, part)
        return remote(ref, ref, hid_send.at[0], hid_side.at[s], (e, sibling))

    def hidden_bytes(s, blocks):
        return hidden.at[s, :, pl.ds(0, blocks * ff_local)]

    def give_back(s, at):
        here, there = results.at[s, :, at], returned.at[e, :, at]
        return remote(here, there, ret_send.at[0], ret_recv.at[e], (s, q))

    inputs = [
        pltpu.make_async_copy(there, here, input_sem.at[i])
        for i, (there, here) in enumerate(
            (
                (value_h, value),
                (gate_h, gate),
                (taps_h, taps),
                (ids_h, ids),
                (logits_h, logits),
                (prob_h, prob),
                (gain_h, gain),
                (proj_h, proj),
                (resid_h, resid),
            )
        )
    ]
    loads = []
    for i, (there, here) in enumerate(((w_gate, gate_v), (w_up, up_v))):
        for t in range(n_tp):
            at = (t % 2 * n_y + t // 2) * width
            loads.append(
                pltpu.make_async_copy(
                    there.at[0, pl.ds(t * width, width)],
                    here.at[pl.ds(at, width)],
                    load_sem.at[i],
                )
            )
    loads.append(pltpu.make_async_copy(w_down.at[0], down_v, load_sem.at[2]))
    for copy in inputs:
        copy.start()
    barrier = pltpu.get_barrier_semaphore()

    @pl.loop(1, n_sp)
    def _(v):
        pl.semaphore_signal(barrier, inc=1, device_id=(moved(v), q), device_id_type=MESH)

    for o in range(1, n_tp):
        pl.semaphore_signal(
            barrier, inc=1, device_id=(e, lax.rem(q + o, n_tp)), device_id_type=MESH
        )
    for copy in inputs[:3]:
        copy.wait()
    for load in loads:
        load.start()

    flow = value[...].astype(jnp.float32) / (1.0 + jnp.exp(-gate[...].astype(jnp.float32)))
    flow = jnp.transpose(flow).astype(jnp.bfloat16)
    halo_out[...] = flow[tokens - history :]
    padded[history:] = flow.astype(jnp.float32)
    lane = lax.broadcasted_iota(jnp.int32, (history, 128), 1)

    def convolve(first):
        filtered = jnp.zeros((history, local), jnp.float32)
        for j in range(taken):
            at = first + history - (taken - 1) + j
            filtered = filtered + taps[j : j + 1] * padded[at : at + history]
        one = jnp.sum(filtered, axis=1, keepdims=True)
        two = jnp.sum(filtered * filtered, axis=1, keepdims=True)
        sums[first : first + history] = jnp.where(lane == 0, one, jnp.where(lane == 1, two, 0.0))
        act[q, first : first + history] = (filtered - one / local).astype(act.dtype)

    sums[0:history] = jnp.zeros((history, 128), jnp.float32)
    for first in range(history, middle, history):
        convolve(first)
    pl.semaphore_wait(barrier, n_sp - 1 + n_tp - 1)

    @pl.when(e + 1 < n_sp)
    def _():
        hand_on().start()

    for j in range(n_y - 1, -1, -1):
        piece(0, j).start()
    for first in range(first + history, tokens, history):
        convolve(first)
    for copy in inputs[3:]:
        copy.wait()
    stats[q] = jnp.transpose(sums[...])[0:8]
    stats[q, 2:3, 0:local] = gain[...]
    for o in range(1, n_tp):
        tell_stats(o).start()
    for j in range(n_y - 1, -1, -1):
        piece(1, j).start()

    ahead = lax.broadcasted_iota(jnp.int32, (tokens, tokens), 0)
    after = lax.broadcasted_iota(jnp.int32, (tokens, tokens), 1)
    lanes = max(128, n_sp)
    row_no = lax.broadcasted_iota(jnp.int32, (lanes, tokens), 0)
    row_hit = [jnp.where(row_no == ids[r : r + 1], 1.0, 0.0) for r in range(top)]
    row_rank = jnp.dot(
        sum(row_hit).astype(jnp.bfloat16),
        jnp.where(ahead < after, 1.0, 0.0).astype(jnp.bfloat16),
        preferred_element_type=jnp.float32,
    )
    slot_rows = [
        (ids[r : r + 1] * capacity).astype(jnp.float32)
        + jnp.sum(row_hit[r] * row_rank, axis=0, keepdims=True)
        for r in range(top)
    ]
    for r in range(top):
        slots[r : r + 1] = slot_rows[r]
    slots[top:] = jnp.zeros((slots.shape[0] - top, tokens), jnp.float32)
    share_slots().start()
    scores = logits[...]
    scores = jnp.exp(scores - jnp.max(scores, axis=0, keepdims=True))
    scores = prob[...] * scores / jnp.sum(scores, axis=0, keepdims=True)
    weights[...] = jnp.transpose(sum(row_hit[r] * scores[r : r + 1] for r in range(top)))

    @pl.when(e > 0)
    def _():
        hand_on().wait_recv()
        padded[0:history] = halo_in[...].astype(jnp.float32)

    @pl.when(e == 0)
    def _():
        padded[0:history] = jnp.zeros_like(halo_in).astype(jnp.float32)

    convolve(0)
    stats_head[q] = jnp.transpose(jnp.concatenate([sums[0:history]] * (128 // history), axis=0))[0:8]
    for o in range(1, n_tp):
        tell_head(o).start()
        tell_last(o).start()

    @pl.loop(0, n_sp)
    def _(x):
        place = (x * capacity + lax.broadcasted_iota(jnp.int32, (capacity, tokens), 0)).astype(
            jnp.float32
        )
        chosen = jnp.zeros((capacity, tokens), jnp.float32)
        for r in range(top):
            chosen = chosen + jnp.where(place == slot_rows[r], 1.0, 0.0)
        picks[x] = chosen.astype(picks.dtype)
        picks_back[x] = jnp.transpose(chosen).astype(picks.dtype)

    total[...] = jnp.zeros_like(total)
    channels = proj.shape[0]

    def moments(table, into, turned):
        one = table[0, 0:1]
        two = table[0, 1:2]
        for t in range(1, n_tp):
            one = one + table[t, 0:1]
            two = two + table[t, 1:2]
        mean = one / channels
        scale = lax.rsqrt(two / channels - mean * mean + 1e-05)
        into[...] = jnp.zeros_like(into)
        for t in range(n_tp):
            into[t : t + 1] = (table[t, 0:1] / local - mean) * scale
        into[n_tp : n_tp + 1] = scale
        turned[...] = jnp.transpose(into[...])

    def norm(first, size, turned):
        for t in range(n_tp):
            scaled = act[t, first : first + size].astype(jnp.float32)
            scaled = scaled * turned[first : first + size, n_tp : n_tp + 1]
            scaled = (scaled + turned[first : first + size, t : t + 1]) * stats[t, 2:3, 0:local]
            scaled = scaled / (1.0 + jnp.exp(-scaled))
            normal[first : first + size, t * local : (t + 1) * local] = scaled.astype(normal.dtype)

    arrived(all_stats, stat_recv.at[0])
    moments(stats, flip, columns)
    for p in range(2):
        for j in range(1, n_y):
            arrived(piece_at(p, 2 * below(j) + core), act_recv.at[p, j - 1])
            pass_piece(p, j).start()
    for p in range(2):
        first, size = pieces[p]
        arrived(act.at[pl.ds(0, n_y), pl.ds(first, size)], act_side.at[p])
        step = 56 if size % 56 == 0 else 16
        for at in range(first, first + size, step):
            norm(at, step, columns)
    arrived(all_last, last_recv.at[0])
    arrived(all_heads, head_recv.at[0])
    moments(stats_head, flip_head, columns_head)
    norm(0, history, columns_head)
    mixed[...] = (
        resid[...].astype(jnp.float32)
        + jnp.dot(normal[...], proj[...], preferred_element_type=jnp.float32)
    ).astype(mixed.dtype)

    def pick(x, block):
        got = jnp.dot(picks[x], block, preferred_element_type=jnp.float32)
        return got.astype(outgoing.dtype)

    for j in range(1, n_y):
        share_front(j).start()

    def send(v, kind):
        outgoing[v] = pick(moved(v), mixed[...])
        dispatch(v, e, kind).start()

    def send_front(v):
        for j in range(1, n_y):
            outgoing_front[j - 1, v] = pick(moved(v), mixed_front[above(j)])
            dispatch_front(v, e, j).start()

    def pick_far(d, block):
        got = jnp.dot(picks_far[d], block, preferred_element_type=jnp.float32)
        return got.astype(outgoing.dtype)

    def forward(d):
        outgoing[far_by + d] = pick_far(d, tok[...])
        dispatch(far_by + d, partner, 1).start()

    def forward_front(d):
        for j in range(1, n_y):
            outgoing_front[j - 1, far_by + d] = pick_far(d, tok_front[above(j)])
            dispatch_front(far_by + d, partner, j).start()

    pl.loop(1, near + 1)(functools.partial(send, kind=0))
    share_tokens().start()
    pl.loop(near + 1, far_by)(functools.partial(send, kind=1))
    quarter(e, y, 0, width)[...] = pick(e, mixed[...])
    share_slots().wait_recv()

    @pl.loop(0, far_by)
    def _(d):
        place = moved(d) * capacity + lax.broadcasted_iota(jnp.int32, (capacity, tokens), 0)
        chosen = jnp.zeros((capacity, tokens), jnp.float32)
        for r in range(top):
            chosen = chosen + jnp.where(place.astype(jnp.float32) == slots_far[r : r + 1], 1.0, 0.0)
        picks_far[d] = chosen.astype(picks_far.dtype)

    def begin(k):
        s = source(k)
        arrived(quarter(s, y, 0, width), whole_recv.at[s])
        for j in range(1, n_y):
            cross(k, j).start()

    def gather(k):
        s = source(k)

        @pl.when(k < near)
        def _():
            for j in range(1, n_y):
                arrived(quarter(s, below(j), 0, width), cross_recv.at[k, j - 1])

        @pl.when((k >= near) & (s != e) & (s != partner))
        def _():
            arrived(half(s, core), whole_recv.at[s])

        halve(s).start()

    for k in range(near):
        begin(k)
    arrived(all_fronts, front_recv.at[0])
    pl.loop(near + 1, far_by)(send_front)
    for j in range(1, n_y):
        of = below(j)
        quarter(e, of, 0, width)[...] = pick(e, mixed_front[of])
    gather(0)
    for j in range(1, n_y):
        share_tokens_front(j).start()
    arrived(gate_v, load_sem.at[0])
    arrived(up_v, load_sem.at[1])
    loads[-1].wait()

    tile = min(256, ff_part)
    out_tile = min(256, width)

    def up_step(s):
        @pl.loop(0, parts)
        def _(part):
            @pl.loop(0, ff_part // tile)
            def _(i):
                first = part * ff_part + i * tile
                at = pl.ds(pl.multiple_of(first, tile), tile)
                g = jnp.dot(rows[s], gate_v[:, at], preferred_element_type=jnp.float32)
                u = jnp.dot(rows[s], up_v[:, at], preferred_element_type=jnp.float32)
                h = (g / (1.0 + jnp.exp(-g)) * u).astype(hidden.dtype)
                hidden[s, :, pl.ds(pl.multiple_of(q * ff_local + first, tile), tile)] = h

            for j in range(1, n_y):
                share(s, part, j).start()
            share(s, part, 0).start()

    def down_step(s):
        @pl.loop(0, width // out_tile)
        def _(i):
            at = pl.ds(pl.multiple_of(i * out_tile, out_tile), out_tile)
            o = jnp.dot(hidden[s], down_v[:, at], preferred_element_type=jnp.float32)
            results[s, :, at] = o.astype(results.dtype)

            @pl.when(s != e)
            def _():
                give_back(s, at).start()

    slot_lane = lax.broadcasted_iota(jnp.int32, weights.shape, 1)

    def combine(x, block):
        got = jnp.dot(picks_back[x], block, preferred_element_type=jnp.float32)
        weight = jnp.sum(jnp.where(slot_lane == x, weights[...], 0.0), axis=1, keepdims=True)
        total[...] += weight * got

    def take(k):
        x = source(k)
        arrived(returned.at[x], ret_recv.at[x])
        combine(x, returned[x])

    @pl.loop(2, n_sp + 4)
    def _(i):
        @pl.when(i == n_sp + 3)
        def _():
            take(n_sp - 3)

        @pl.when(i < n_sp + 2)
        def _():
            s = source(i - 2)
            arrived(half(s, 1 - core), half_recv.at[s])
            up_step(s)

        @pl.when(i == 3)
        def _():
            arrived(tok, tok_sem.at[1])
            quarter(partner, y, 0, width)[...] = pick_far(0, tok[...])
            pl.loop(1, far_by - 1)(forward)

        @pl.when(i == 4)
        def _():
            arrived(all_tokens, tok_recv.at[0])
            for j in range(1, n_y):
                of = below(j)
                quarter(partner, of, 0, width)[...] = pick_far(0, tok_front[of])
            forward(far_by - 1)
            pl.loop(1, far_by - 1)(forward_front)

        @pl.when(i == 5)
        def _():
            forward_front(far_by - 1)

        @pl.when(i >= 4)
        def _():
            s = source(i - 4)
            arrived(hidden_bytes(s, n_y), hid_side.at[s])
            down_step(s)

            @pl.when(i == n_sp + 3)
            def _():
                combine(e, results[e])

        @pl.when(i < n_sp + 1)
        def _():
            gather(i - 1)

        @pl.when((i >= 3) & (i < n_sp + 3))
        def _():
            s = source(i - 3)
            for part in range(parts):
                for j in range(1, n_y):
                    t = 2 * below(j) + core
                    arrived(hidden_at(s, t, part), hid_recv.at[s, j - 1, part])
                    pass_on(s, part, j).start()

        @pl.when((i >= 6) & (i < n_sp + 3))
        def _():
            take(i - 6)

    for k in range(max(0, n_sp - 2), n_sp - 1):
        take(k)
    out[...] = (mixed[...].astype(jnp.float32) + total[...]).astype(out.dtype)

    every = pl.ds(0, n_sp)
    for k in range(near):
        for j in range(1, n_y):
            cross(k, j).wait_send()
    arrived(outgoing.at[pl.ds(0, near)], whole_send.at[0])
    rest = pl.ds(0, n_sp - 2 - near)
    arrived(rows.at[rest, :, pl.ds(0, n_y * width)], whole_send.at[1])
    arrived(rows.at[every, :, pl.ds(0, n_y * width)], half_send.at[0])
    arrived(hidden.at[every, :, pl.ds(0, (2 * n_y - 1) * ff_local)], hid_send.at[0])
    arrived(results.at[pl.ds(0, n_sp - 1)], ret_send.at[0])

    @pl.when(e + 1 < n_sp)
    def _():
        hand_on().wait_send()

    arrived(all_stats, stat_send.at[0])
    arrived(all_last, last_send.at[0])
    arrived(all_heads, head_send.at[0])
    arrived(all_pieces, act_send.at[0])
    share_slots().wait_send()
    share_tokens().wait_send()
    arrived(all_fronts, front_send.at[0])
    arrived(all_tokens, tok_send.at[0])


def run_layer(value, gate, taps, gain, proj, resid, ids, logits, prob, w_gate, w_up, w_down):
    n_sp, n_tp = lax.axis_size("sp"), lax.axis_size("tp")
    n_y = n_tp // 2
    tokens, width = resid.shape
    local = value.shape[0]
    capacity = 4 * tokens // n_sp
    ff_local = w_gate.shape[2]
    history = -(-(taps.shape[0] - 1) // 16) * 16
    parts = 4 if ff_local % 1024 == 0 else 1
    lanes = max(128, n_sp)
    dma = pltpu.SemaphoreType.DMA
    small = (value, gate, taps, gain, proj, resid, ids, logits, prob)
    return pl.pallas_call(
        functools.partial(expert_kernel, n_sp, n_tp),
        out_shape=pltpu.VMEM(resid.shape, resid.dtype),
        in_specs=[pl.BlockSpec(memory_space=pltpu.HBM)] * 12,
        out_specs=pl.BlockSpec(memory_space=pltpu.VMEM),
        scratch_shapes=[pltpu.VMEM(x.shape, x.dtype) for x in small]
        + [
            pltpu.VMEM((history + tokens, local), jnp.float32),
            pltpu.VMEM((tokens, 128), jnp.float32),
            pltpu.VMEM((history, local), jnp.bfloat16),
            pltpu.VMEM((history, local), jnp.bfloat16),
            pltpu.VMEM((n_tp, 8, tokens), jnp.float32),
            pltpu.VMEM((n_tp, 8, 128), jnp.float32),
            pltpu.VMEM((128, tokens), jnp.float32),
            pltpu.VMEM((tokens, 128), jnp.float32),
            pltpu.VMEM((128, 128), jnp.float32),
            pltpu.VMEM((128, 128), jnp.float32),
            pltpu.VMEM((n_tp, tokens, local), jnp.bfloat16),
            pltpu.VMEM((tokens, local * n_tp), jnp.bfloat16),
            pltpu.VMEM((tokens, width), jnp.bfloat16),
            pltpu.VMEM((n_y, tokens, width), jnp.bfloat16),
            pltpu.VMEM((8, tokens), jnp.float32),
            pltpu.VMEM((8, tokens), jnp.float32),
            pltpu.VMEM((tokens, width), jnp.bfloat16),
            pltpu.VMEM((n_y, tokens, width), jnp.bfloat16),
            pltpu.VMEM((n_sp, capacity, tokens), jnp.bfloat16),
            pltpu.VMEM((n_sp // 2, capacity, tokens), jnp.bfloat16),
            pltpu.VMEM((n_sp, tokens, capacity), jnp.bfloat16),
            pltpu.VMEM((tokens, lanes), jnp.float32),
            pltpu.VMEM((tokens, width), jnp.float32),
            pltpu.VMEM((n_sp, capacity, width), jnp.bfloat16),
            pltpu.VMEM((n_y - 1, n_sp, capacity, width), jnp.bfloat16),
            pltpu.VMEM((n_sp, capacity, width * n_tp), jnp.bfloat16),
            pltpu.VMEM((n_sp, capacity, ff_local * n_tp), jnp.bfloat16),
            pltpu.VMEM((n_sp, capacity, width), jnp.bfloat16),
            pltpu.VMEM((n_sp, capacity, width), jnp.bfloat16),
            pltpu.VMEM(w_gate.shape[1:], jnp.bfloat16),
            pltpu.VMEM(w_up.shape[1:], jnp.bfloat16),
            pltpu.VMEM(w_down.shape[1:], jnp.bfloat16),
            dma((len(small),)),
            dma((3,)),
            dma((2,)),
        ]
        + [dma((1,))] * 6
        + [
            dma((2, n_y - 1)),
            dma((2,)),
            dma((1,)),
            dma((1,)),
            dma((1,)),
            dma((2,)),
            dma((2,)),
            dma((1,)),
            dma((1,)),
            dma((2,)),
            dma((n_sp,)),
            dma((2, n_y - 1)),
            dma((2, n_y - 1)),
            dma((1,)),
            dma((n_sp,)),
            dma((n_sp, n_y - 1, parts)),
            dma((n_sp,)),
            dma((1,)),
            dma((1,)),
            dma((n_sp,)),
        ],
        compiler_params=pltpu.CompilerParams(
            collective_id=0, has_side_effects=True, vmem_limit_bytes=57000000
        ),
    )(*small, w_gate, w_up, w_down)


def per_device(
    glu_value,
    glu_gate,
    conv_taps,
    norm_gain,
    out_proj,
    resid,
    expert_ids,
    route_logits,
    group_prob,
    w_gate,
    w_up,
    w_down,
):
    return run_layer(
        glu_value,
        glu_gate,
        conv_taps.T,
        norm_gain[None, :],
        out_proj,
        resid,
        expert_ids.T,
        route_logits.T,
        group_prob[None, :],
        w_gate,
        w_up,
        w_down,
    )


def solution(mesh):
    return jax.shard_map(
        per_device,
        mesh=mesh,
        in_specs=(
            P("tp", "sp"),
            P("tp", "sp"),
            P("tp", None),
            P("tp"),
            P(None, "tp"),
            P("sp", "tp"),
            P("sp", None),
            P("sp", None),
            P("sp"),
            P("sp", None, "tp"),
            P("sp", None, "tp"),
            P("sp", None, "tp"),
        ),
        out_specs=P("sp", "tp"),
        check_vma=False,
    )
```

```python
import functools

import jax
import jax.numpy as jnp
from jax import lax
from jax.experimental import pallas as pl
from jax.experimental.pallas import tpu as pltpu
from jax.sharding import PartitionSpec as P

MESH = pl.DeviceIdType.MESH


def expert_kernel(
    n_sp,
    n_tp,
    value_h,
    gate_h,
    taps_h,
    gain_h,
    proj_h,
    resid_h,
    ids_h,
    logits_h,
    prob_h,
    w_gate,
    w_up,
    w_down,
    out,
    value,
    gate,
    taps,
    gain,
    proj,
    resid,
    ids,
    logits,
    prob,
    padded,
    sums,
    halo_out,
    halo_in,
    stats,
    stats_head,
    flip,
    columns,
    flip_head,
    columns_head,
    act,
    normal,
    mixed,
    mixed_front,
    slots,
    slots_far,
    tok,
    tok_front,
    picks,
    picks_far,
    picks_back,
    weights,
    total,
    outgoing,
    outgoing_front,
    rows,
    hidden,
    results,
    returned,
    gate_v,
    up_v,
    down_v,
    input_sem,
    load_sem,
    halo_sem,
    stat_send,
    stat_recv,
    head_send,
    head_recv,
    last_send,
    last_recv,
    act_recv,
    act_side,
    act_send,
    front_send,
    front_recv,
    slot_sem,
    tok_sem,
    tok_send,
    tok_recv,
    whole_send,
    whole_recv,
    cross_send,
    cross_recv,
    half_send,
    half_recv,
    hid_recv,
    hid_side,
    hid_send,
    ret_send,
    ret_recv,
):
    e = lax.axis_index("sp")
    q = lax.axis_index("tp")
    n_y = n_tp // 2
    y, core = q // 2, q % 2
    sibling = 2 * y + (1 - core)
    _, capacity, width = results.shape
    tokens = mixed.shape[0]
    ff_local = gate_v.shape[1]
    parts = hid_recv.shape[2]
    near = cross_send.shape[0]
    ff_part = ff_local // parts
    history, local = halo_in.shape
    taken = taps.shape[0]
    top = ids.shape[0]
    middle = history + (tokens - history) // 32 * 16
    pieces = ((history, middle - history), (middle, tokens - middle))
    far_by = n_sp // 2
    bits = [e // 2**b % 2 for b in range(n_sp.bit_length() - 1)]

    def moved(v):
        return sum((bits[b] + v // 2**b) % 2 * 2**b for b in range(len(bits)))

    def order(k):
        return lax.rem(k + 1, n_sp)

    def source(k):
        return moved(order(k))

    partner = moved(far_by)

    def far(j):
        return 2 * lax.rem(y + j, n_y) + core

    def above(j):
        return lax.rem(y + j, n_y)

    def below(j):
        return lax.rem(y + n_y - j, n_y)

    def quarter(s, of, first, size):
        at = pl.multiple_of((core * n_y + of) * width + first, min(128, width))
        return rows.at[s, :, pl.ds(at, size)]

    def half(s, c):
        return rows.at[s, :, pl.ds(pl.multiple_of(c * n_y * width, width), n_y * width)]

    def hidden_at(s, t, part):
        at = pl.multiple_of(t * ff_local + part * ff_part, ff_part)
        return hidden.at[s, :, pl.ds(at, ff_part)]

    def remote(src, dst, send, recv, to):
        return pltpu.make_async_remote_copy(
            src_ref=src,
            dst_ref=dst,
            send_sem=send,
            recv_sem=recv,
            device_id=to,
            device_id_type=MESH,
        )

    def arrived(ref, recv):
        pltpu.make_async_copy(ref, ref, recv).wait()

    def tell(o, ref, send, recv):
        return remote(ref, ref, send.at[0], recv.at[0], (e, lax.rem(q + o, n_tp)))

    def tell_stats(o):
        return tell(o, stats.at[q], stat_send, stat_recv)

    def tell_last(o):
        return tell(o, stats_head.at[q], last_send, last_recv)

    def tell_head(o):
        return tell(o, act.at[q, pl.ds(0, history)], head_send, head_recv)

    others = pl.ds(0, n_tp - 1)
    sent = pl.ds(0, 2 * n_y - 1)
    all_stats = stats.at[others]
    all_last = stats_head.at[others]
    all_heads = act.at[others, pl.ds(0, history)]
    all_pieces = act.at[sent, pl.ds(history, tokens - history)]

    def hand_on():
        to = (lax.rem(e + 1, n_sp), q)
        return remote(halo_out, halo_in, halo_sem.at[0], halo_sem.at[1], to)

    def piece_at(p, t):
        return act.at[t, pl.ds(pieces[p][0], pieces[p][1])]

    def piece(p, j):
        ref = piece_at(p, q)
        if j == 0:
            return remote(ref, ref, act_send.at[0], act_side.at[p], (e, sibling))
        return remote(ref, ref, act_send.at[0], act_recv.at[p, j - 1], (e, far(j)))

    def pass_piece(p, j):
        ref = piece_at(p, 2 * below(j) + core)
        return remote(ref, ref, act_send.at[0], act_side.at[p], (e, sibling))

    def share_front(j, at):
        here, there = mixed.at[:, at], mixed_front.at[y, :, at]
        return remote(here, there, front_send.at[0], front_recv.at[0], (e, far(j)))

    all_fronts = mixed_front.at[pl.ds(0, n_y - 1)]

    def share_slots():
        return remote(slots, slots_far, slot_sem.at[0], slot_sem.at[1], (partner, q))

    def share_tokens():
        return remote(mixed, tok, tok_sem.at[0], tok_sem.at[1], (partner, q))

    def share_tokens_front(j):
        of = above(j)
        ours = mixed_front.at[of]
        return remote(ours, tok_front.at[of], tok_send.at[0], tok_recv.at[0], (partner, q))

    all_tokens = tok_front.at[pl.ds(0, n_y - 1)]

    def dispatch(v, s, kind):
        to = moved(lax.rem(v, far_by))
        return remote(
            outgoing.at[v],
            quarter(s, y, 0, width),
            whole_send.at[kind],
            whole_recv.at[s],
            (to, q),
        )

    def dispatch_front(v, s, j):
        to = moved(lax.rem(v, far_by))
        of = above(j)
        return remote(
            outgoing_front.at[j - 1, v],
            quarter(s, of, 0, width),
            whole_send.at[1],
            whole_recv.at[s],
            (to, q),
        )

    def cross(k, j):
        ref = quarter(source(k), y, 0, width)
        return remote(ref, ref, cross_send.at[k, j - 1], cross_recv.at[k, j - 1], (e, far(j)))

    def halve(s):
        ref = half(s, core)
        return remote(ref, ref, half_send.at[0], half_recv.at[s], (e, sibling))

    def share(s, part, j):
        ref = hidden_at(s, q, part)
        if j == 0:
            return remote(ref, ref, hid_send.at[0], hid_side.at[s], (e, sibling))
        return remote(ref, ref, hid_send.at[0], hid_recv.at[s, j - 1, part], (e, far(j)))

    def pass_on(s, part, j):
        ref = hidden_at(s, 2 * below(j) + core, part)
        return remote(ref, ref, hid_send.at[0], hid_side.at[s], (e, sibling))

    def hidden_bytes(s, blocks):
        return hidden.at[s, :, pl.ds(0, blocks * ff_local)]

    def give_back(s, at):
        here, there = results.at[s, :, at], returned.at[e, :, at]
        return remote(here, there, ret_send.at[0], ret_recv.at[e], (s, q))

    inputs = [
        pltpu.make_async_copy(there, here, input_sem.at[i])
        for i, (there, here) in enumerate(
            (
                (value_h, value),
                (gate_h, gate),
                (taps_h, taps),
                (ids_h, ids),
                (logits_h, logits),
                (prob_h, prob),
                (gain_h, gain),
                (proj_h, proj),
                (resid_h, resid),
            )
        )
    ]
    loads = []
    for i, (there, here) in enumerate(((w_gate, gate_v), (w_up, up_v))):
        for t in range(n_tp):
            at = (t % 2 * n_y + t // 2) * width
            loads.append(
                pltpu.make_async_copy(
                    there.at[0, pl.ds(t * width, width)],
                    here.at[pl.ds(at, width)],
                    load_sem.at[i],
                )
            )
    loads.append(pltpu.make_async_copy(w_down.at[0], down_v, load_sem.at[2]))
    for copy in inputs:
        copy.start()
    barrier = pltpu.get_barrier_semaphore()

    @pl.loop(1, n_sp)
    def _(v):
        pl.semaphore_signal(barrier, inc=1, device_id=(moved(v), q), device_id_type=MESH)

    for o in range(1, n_tp):
        pl.semaphore_signal(
            barrier, inc=1, device_id=(e, lax.rem(q + o, n_tp)), device_id_type=MESH
        )
    for copy in inputs[:3]:
        copy.wait()
    for load in loads:
        load.start()

    flow = value[...].astype(jnp.float32) / (1.0 + jnp.exp(-gate[...].astype(jnp.float32)))
    flow = jnp.transpose(flow).astype(jnp.bfloat16)
    halo_out[...] = flow[tokens - history :]
    padded[history:] = flow.astype(jnp.float32)
    lane = lax.broadcasted_iota(jnp.int32, (history, 128), 1)

    def convolve(first):
        filtered = jnp.zeros((history, local), jnp.float32)
        for j in range(taken):
            at = first + history - (taken - 1) + j
            filtered = filtered + taps[j : j + 1] * padded[at : at + history]
        one = jnp.sum(filtered, axis=1, keepdims=True)
        two = jnp.sum(filtered * filtered, axis=1, keepdims=True)
        sums[first : first + history] = jnp.where(lane == 0, one, jnp.where(lane == 1, two, 0.0))
        act[q, first : first + history] = (filtered - one / local).astype(act.dtype)

    sums[0:history] = jnp.zeros((history, 128), jnp.float32)
    for first in range(history, middle, history):
        convolve(first)
    pl.semaphore_wait(barrier, n_sp - 1 + n_tp - 1)

    @pl.when(e + 1 < n_sp)
    def _():
        hand_on().start()

    for j in range(n_y - 1, -1, -1):
        piece(0, j).start()
    for first in range(first + history, tokens, history):
        convolve(first)
    for copy in inputs[3:]:
        copy.wait()
    stats[q] = jnp.transpose(sums[...])[0:8]
    stats[q, 2:3, 0:local] = gain[...]
    for o in range(1, n_tp):
        tell_stats(o).start()
    for j in range(n_y - 1, -1, -1):
        piece(1, j).start()

    ahead = lax.broadcasted_iota(jnp.int32, (tokens, tokens), 0)
    after = lax.broadcasted_iota(jnp.int32, (tokens, tokens), 1)
    lanes = max(128, n_sp)
    row_no = lax.broadcasted_iota(jnp.int32, (lanes, tokens), 0)
    row_hit = [jnp.where(row_no == ids[r : r + 1], 1.0, 0.0) for r in range(top)]
    row_rank = jnp.dot(
        sum(row_hit).astype(jnp.bfloat16),
        jnp.where(ahead < after, 1.0, 0.0).astype(jnp.bfloat16),
        preferred_element_type=jnp.float32,
    )
    slot_rows = [
        (ids[r : r + 1] * capacity).astype(jnp.float32)
        + jnp.sum(row_hit[r] * row_rank, axis=0, keepdims=True)
        for r in range(top)
    ]
    for r in range(top):
        slots[r : r + 1] = slot_rows[r]
    slots[top:] = jnp.zeros((slots.shape[0] - top, tokens), jnp.float32)
    share_slots().start()
    scores = logits[...]
    scores = jnp.exp(scores - jnp.max(scores, axis=0, keepdims=True))
    scores = prob[...] * scores / jnp.sum(scores, axis=0, keepdims=True)
    weights[...] = jnp.transpose(sum(row_hit[r] * scores[r : r + 1] for r in range(top)))

    @pl.when(e > 0)
    def _():
        hand_on().wait_recv()
        padded[0:history] = halo_in[...].astype(jnp.float32)

    @pl.when(e == 0)
    def _():
        padded[0:history] = jnp.zeros_like(halo_in).astype(jnp.float32)

    convolve(0)
    stats_head[q] = jnp.transpose(jnp.concatenate([sums[0:history]] * (128 // history), axis=0))[0:8]
    for o in range(1, n_tp):
        tell_head(o).start()
        tell_last(o).start()

    @pl.loop(0, n_sp)
    def _(x):
        place = (x * capacity + lax.broadcasted_iota(jnp.int32, (capacity, tokens), 0)).astype(
            jnp.float32
        )
        chosen = jnp.zeros((capacity, tokens), jnp.float32)
        for r in range(top):
            chosen = chosen + jnp.where(place == slot_rows[r], 1.0, 0.0)
        picks[x] = chosen.astype(picks.dtype)
        picks_back[x] = jnp.transpose(chosen).astype(picks.dtype)

    total[...] = jnp.zeros_like(total)
    channels = proj.shape[0]

    def moments(table, into, turned):
        one = table[0, 0:1]
        two = table[0, 1:2]
        for t in range(1, n_tp):
            one = one + table[t, 0:1]
            two = two + table[t, 1:2]
        mean = one / channels
        scale = lax.rsqrt(two / channels - mean * mean + 1e-05)
        into[...] = jnp.zeros_like(into)
        for t in range(n_tp):
            into[t : t + 1] = (table[t, 0:1] / local - mean) * scale
        into[n_tp : n_tp + 1] = scale
        turned[...] = jnp.transpose(into[...])

    def norm(first, size, turned):
        for t in range(n_tp):
            scaled = act[t, first : first + size].astype(jnp.float32)
            scaled = scaled * turned[first : first + size, n_tp : n_tp + 1]
            scaled = (scaled + turned[first : first + size, t : t + 1]) * stats[t, 2:3, 0:local]
            scaled = scaled / (1.0 + jnp.exp(-scaled))
            normal[first : first + size, t * local : (t + 1) * local] = scaled.astype(normal.dtype)

    arrived(all_stats, stat_recv.at[0])
    moments(stats, flip, columns)
    for p in range(2):
        for j in range(1, n_y):
            arrived(piece_at(p, 2 * below(j) + core), act_recv.at[p, j - 1])
            pass_piece(p, j).start()
    for p in range(2):
        first, size = pieces[p]
        arrived(act.at[pl.ds(0, n_y), pl.ds(first, size)], act_side.at[p])
        step = 56 if size % 56 == 0 else 16
        for at in range(first, first + size, step):
            norm(at, step, columns)
    arrived(all_last, last_recv.at[0])
    arrived(all_heads, head_recv.at[0])
    moments(stats_head, flip_head, columns_head)
    norm(0, history, columns_head)
    strip = 256 if width % 256 == 0 else width
    for first in range(0, width, strip):
        at = pl.ds(first, strip)
        sums_at = jnp.dot(normal[...], proj[:, at], preferred_element_type=jnp.float32)
        mixed[:, at] = (resid[:, at].astype(jnp.float32) + sums_at).astype(mixed.dtype)
        for j in range(1, n_y):
            share_front(j, at).start()

    def pick(x, block):
        got = jnp.dot(picks[x], block, preferred_element_type=jnp.float32)
        return got.astype(outgoing.dtype)


    def send(v, kind):
        outgoing[v] = pick(moved(v), mixed[...])
        dispatch(v, e, kind).start()

    def send_front(v):
        for j in range(1, n_y):
            outgoing_front[j - 1, v] = pick(moved(v), mixed_front[above(j)])
            dispatch_front(v, e, j).start()

    def pick_far(d, block):
        got = jnp.dot(picks_far[d], block, preferred_element_type=jnp.float32)
        return got.astype(outgoing.dtype)

    def forward(d):
        outgoing[far_by + d] = pick_far(d, tok[...])
        dispatch(far_by + d, partner, 1).start()

    def forward_front(d):
        for j in range(1, n_y):
            outgoing_front[j - 1, far_by + d] = pick_far(d, tok_front[above(j)])
            dispatch_front(far_by + d, partner, j).start()

    pl.loop(1, near + 1)(functools.partial(send, kind=0))
    share_tokens().start()
    pl.loop(near + 1, far_by)(functools.partial(send, kind=1))
    quarter(e, y, 0, width)[...] = pick(e, mixed[...])
    share_slots().wait_recv()

    @pl.loop(0, far_by)
    def _(d):
        place = moved(d) * capacity + lax.broadcasted_iota(jnp.int32, (capacity, tokens), 0)
        chosen = jnp.zeros((capacity, tokens), jnp.float32)
        for r in range(top):
            chosen = chosen + jnp.where(place.astype(jnp.float32) == slots_far[r : r + 1], 1.0, 0.0)
        picks_far[d] = chosen.astype(picks_far.dtype)

    def begin(k):
        s = source(k)
        arrived(quarter(s, y, 0, width), whole_recv.at[s])
        for j in range(1, n_y):
            cross(k, j).start()

    def gather(k):
        s = source(k)

        @pl.when(k < near)
        def _():
            for j in range(1, n_y):
                arrived(quarter(s, below(j), 0, width), cross_recv.at[k, j - 1])

        @pl.when((k >= near) & (s != e) & (s != partner))
        def _():
            arrived(half(s, core), whole_recv.at[s])

        halve(s).start()

    for k in range(near):
        begin(k)
    arrived(all_fronts, front_recv.at[0])
    pl.loop(near + 1, far_by)(send_front)
    for j in range(1, n_y):
        of = below(j)
        quarter(e, of, 0, width)[...] = pick(e, mixed_front[of])
    gather(0)
    for j in range(1, n_y):
        share_tokens_front(j).start()
    arrived(gate_v, load_sem.at[0])
    arrived(up_v, load_sem.at[1])
    loads[-1].wait()

    tile = min(256, ff_part)
    out_tile = min(256, width)

    def up_step(s):
        @pl.loop(0, parts)
        def _(part):
            @pl.loop(0, ff_part // tile)
            def _(i):
                first = part * ff_part + i * tile
                at = pl.ds(pl.multiple_of(first, tile), tile)
                g = jnp.dot(rows[s], gate_v[:, at], preferred_element_type=jnp.float32)
                u = jnp.dot(rows[s], up_v[:, at], preferred_element_type=jnp.float32)
                h = (g / (1.0 + jnp.exp(-g)) * u).astype(hidden.dtype)
                hidden[s, :, pl.ds(pl.multiple_of(q * ff_local + first, tile), tile)] = h

            for j in range(1, n_y):
                share(s, part, j).start()
            share(s, part, 0).start()

    def down_step(s):
        @pl.loop(0, width // out_tile)
        def _(i):
            at = pl.ds(pl.multiple_of(i * out_tile, out_tile), out_tile)
            o = jnp.dot(hidden[s], down_v[:, at], preferred_element_type=jnp.float32)
            results[s, :, at] = o.astype(results.dtype)

            @pl.when(s != e)
            def _():
                give_back(s, at).start()

    slot_lane = lax.broadcasted_iota(jnp.int32, weights.shape, 1)

    def combine(x, block):
        got = jnp.dot(picks_back[x], block, preferred_element_type=jnp.float32)
        weight = jnp.sum(jnp.where(slot_lane == x, weights[...], 0.0), axis=1, keepdims=True)
        total[...] += weight * got

    def take(k):
        x = source(k)
        arrived(returned.at[x], ret_recv.at[x])
        combine(x, returned[x])

    @pl.loop(2, n_sp + 4)
    def _(i):
        @pl.when(i == n_sp + 3)
        def _():
            take(n_sp - 3)

        @pl.when(i < n_sp + 2)
        def _():
            s = source(i - 2)
            arrived(half(s, 1 - core), half_recv.at[s])
            up_step(s)

        @pl.when(i == 3)
        def _():
            arrived(tok, tok_sem.at[1])
            quarter(partner, y, 0, width)[...] = pick_far(0, tok[...])
            pl.loop(1, far_by - 1)(forward)

        @pl.when(i == 4)
        def _():
            arrived(all_tokens, tok_recv.at[0])
            for j in range(1, n_y):
                of = below(j)
                quarter(partner, of, 0, width)[...] = pick_far(0, tok_front[of])
            forward(far_by - 1)
            pl.loop(1, far_by - 1)(forward_front)

        @pl.when(i == 5)
        def _():
            forward_front(far_by - 1)

        @pl.when(i >= 4)
        def _():
            s = source(i - 4)
            arrived(hidden_bytes(s, n_y), hid_side.at[s])
            down_step(s)

            @pl.when(i == n_sp + 3)
            def _():
                combine(e, results[e])

        @pl.when(i < n_sp + 1)
        def _():
            gather(i - 1)

        @pl.when((i >= 3) & (i < n_sp + 3))
        def _():
            s = source(i - 3)
            for part in range(parts):
                for j in range(1, n_y):
                    t = 2 * below(j) + core
                    arrived(hidden_at(s, t, part), hid_recv.at[s, j - 1, part])
                    pass_on(s, part, j).start()

        @pl.when((i >= 6) & (i < n_sp + 3))
        def _():
            take(i - 6)

    for k in range(max(0, n_sp - 2), n_sp - 1):
        take(k)
    out[...] = (mixed[...].astype(jnp.float32) + total[...]).astype(out.dtype)

    every = pl.ds(0, n_sp)
    for k in range(near):
        for j in range(1, n_y):
            cross(k, j).wait_send()
    arrived(outgoing.at[pl.ds(0, near)], whole_send.at[0])
    rest = pl.ds(0, n_sp - 2 - near)
    arrived(rows.at[rest, :, pl.ds(0, n_y * width)], whole_send.at[1])
    arrived(rows.at[every, :, pl.ds(0, n_y * width)], half_send.at[0])
    arrived(hidden.at[every, :, pl.ds(0, (2 * n_y - 1) * ff_local)], hid_send.at[0])
    arrived(results.at[pl.ds(0, n_sp - 1)], ret_send.at[0])

    @pl.when(e + 1 < n_sp)
    def _():
        hand_on().wait_send()

    arrived(all_stats, stat_send.at[0])
    arrived(all_last, last_send.at[0])
    arrived(all_heads, head_send.at[0])
    arrived(all_pieces, act_send.at[0])
    share_slots().wait_send()
    share_tokens().wait_send()
    arrived(all_fronts, front_send.at[0])
    arrived(all_tokens, tok_send.at[0])


def run_layer(value, gate, taps, gain, proj, resid, ids, logits, prob, w_gate, w_up, w_down):
    n_sp, n_tp = lax.axis_size("sp"), lax.axis_size("tp")
    n_y = n_tp // 2
    tokens, width = resid.shape
    local = value.shape[0]
    capacity = 4 * tokens // n_sp
    ff_local = w_gate.shape[2]
    history = -(-(taps.shape[0] - 1) // 16) * 16
    parts = 4 if ff_local % 1024 == 0 else 1
    lanes = max(128, n_sp)
    dma = pltpu.SemaphoreType.DMA
    small = (value, gate, taps, gain, proj, resid, ids, logits, prob)
    return pl.pallas_call(
        functools.partial(expert_kernel, n_sp, n_tp),
        out_shape=pltpu.VMEM(resid.shape, resid.dtype),
        in_specs=[pl.BlockSpec(memory_space=pltpu.HBM)] * 12,
        out_specs=pl.BlockSpec(memory_space=pltpu.VMEM),
        scratch_shapes=[pltpu.VMEM(x.shape, x.dtype) for x in small]
        + [
            pltpu.VMEM((history + tokens, local), jnp.float32),
            pltpu.VMEM((tokens, 128), jnp.float32),
            pltpu.VMEM((history, local), jnp.bfloat16),
            pltpu.VMEM((history, local), jnp.bfloat16),
            pltpu.VMEM((n_tp, 8, tokens), jnp.float32),
            pltpu.VMEM((n_tp, 8, 128), jnp.float32),
            pltpu.VMEM((128, tokens), jnp.float32),
            pltpu.VMEM((tokens, 128), jnp.float32),
            pltpu.VMEM((128, 128), jnp.float32),
            pltpu.VMEM((128, 128), jnp.float32),
            pltpu.VMEM((n_tp, tokens, local), jnp.bfloat16),
            pltpu.VMEM((tokens, local * n_tp), jnp.bfloat16),
            pltpu.VMEM((tokens, width), jnp.bfloat16),
            pltpu.VMEM((n_y, tokens, width), jnp.bfloat16),
            pltpu.VMEM((8, tokens), jnp.float32),
            pltpu.VMEM((8, tokens), jnp.float32),
            pltpu.VMEM((tokens, width), jnp.bfloat16),
            pltpu.VMEM((n_y, tokens, width), jnp.bfloat16),
            pltpu.VMEM((n_sp, capacity, tokens), jnp.bfloat16),
            pltpu.VMEM((n_sp // 2, capacity, tokens), jnp.bfloat16),
            pltpu.VMEM((n_sp, tokens, capacity), jnp.bfloat16),
            pltpu.VMEM((tokens, lanes), jnp.float32),
            pltpu.VMEM((tokens, width), jnp.float32),
            pltpu.VMEM((n_sp, capacity, width), jnp.bfloat16),
            pltpu.VMEM((n_y - 1, n_sp, capacity, width), jnp.bfloat16),
            pltpu.VMEM((n_sp, capacity, width * n_tp), jnp.bfloat16),
            pltpu.VMEM((n_sp, capacity, ff_local * n_tp), jnp.bfloat16),
            pltpu.VMEM((n_sp, capacity, width), jnp.bfloat16),
            pltpu.VMEM((n_sp, capacity, width), jnp.bfloat16),
            pltpu.VMEM(w_gate.shape[1:], jnp.bfloat16),
            pltpu.VMEM(w_up.shape[1:], jnp.bfloat16),
            pltpu.VMEM(w_down.shape[1:], jnp.bfloat16),
            dma((len(small),)),
            dma((3,)),
            dma((2,)),
        ]
        + [dma((1,))] * 6
        + [
            dma((2, n_y - 1)),
            dma((2,)),
            dma((1,)),
            dma((1,)),
            dma((1,)),
            dma((2,)),
            dma((2,)),
            dma((1,)),
            dma((1,)),
            dma((2,)),
            dma((n_sp,)),
            dma((2, n_y - 1)),
            dma((2, n_y - 1)),
            dma((1,)),
            dma((n_sp,)),
            dma((n_sp, n_y - 1, parts)),
            dma((n_sp,)),
            dma((1,)),
            dma((1,)),
            dma((n_sp,)),
        ],
        compiler_params=pltpu.CompilerParams(
            collective_id=0, has_side_effects=True, vmem_limit_bytes=57000000
        ),
    )(*small, w_gate, w_up, w_down)


def per_device(
    glu_value,
    glu_gate,
    conv_taps,
    norm_gain,
    out_proj,
    resid,
    expert_ids,
    route_logits,
    group_prob,
    w_gate,
    w_up,
    w_down,
):
    return run_layer(
        glu_value,
        glu_gate,
        conv_taps.T,
        norm_gain[None, :],
        out_proj,
        resid,
        expert_ids.T,
        route_logits.T,
        group_prob[None, :],
        w_gate,
        w_up,
        w_down,
    )


def solution(mesh):
    return jax.shard_map(
        per_device,
        mesh=mesh,
        in_specs=(
            P("tp", "sp"),
            P("tp", "sp"),
            P("tp", None),
            P("tp"),
            P(None, "tp"),
            P("sp", "tp"),
            P("sp", None),
            P("sp", None),
            P("sp"),
            P("sp", None, "tp"),
            P("sp", None, "tp"),
            P("sp", None, "tp"),
        ),
        out_specs=P("sp", "tp"),
        check_vma=False,
    )
```
